256 devices in a mesh: ep: 64 (over z, x, core), tp: 4 (over y).
Axes of the slice: x: 4, y: 4, z: 8, core: 2. Of those that a mesh axis runs over, the one named last changes fastest.
Arguments:
- mix_in: bfloat16 [32768, 2048], P('ep'), may hold values from -6 to 6
- forget_shift: float32 [32768], P('ep'), may hold values from -2.5 to 2.5, as said below
- mix_gain: float32 [2048], replicated, may hold values from 0.1 to 1.9
- w_query: bfloat16 [2048, 1024], P(None, 'tp'), may hold values from -0.125 to 0.125
- w_forget: bfloat16 [2048, 1024], P(None, 'tp'), may hold values from -0.125 to 0.125
- w_value: bfloat16 [2048, 1024], P(None, 'tp'), may hold values from -0.125 to 0.125
- forget_room: float32 [1024], P('tp'), may hold values from 0 to 1, as said below
- head_gain: float32 [1024], P('tp'), may hold values from 0.1 to 1.9
- w_out: bfloat16 [1024, 2048], P('tp'), may hold values from -0.1875 to 0.1875
- moe_in: bfloat16 [16384, 2048], P('ep'), may hold values from -6 to 6
- moe_gain: float32 [2048], replicated, may hold values from 0.1 to 1.9
- expert_choice: int32 [16384, 4], P('ep'), may hold values from 0 to 63, as said below
- route_logit: float32 [16384, 4], P(('ep', 'tp')), may hold values from -6 to 6
- w_exp_gate: bfloat16 [64, 2048, 1024], P('ep', None, 'tp'), may hold values from -0.125 to 0.125
- w_exp_up: bfloat16 [64, 2048, 1024], P('ep', None, 'tp'), may hold values from -0.125 to 0.125
- w_exp_down: bfloat16 [64, 1024, 2048], P('ep', 'tp'), may hold values from -0.1875 to 0.1875
- w_sh_gate: bfloat16 [2048, 512], P(None, 'tp'), may hold values from -0.125 to 0.125
- w_sh_up: bfloat16 [2048, 512], P(None, 'tp'), may hold values from -0.125 to 0.125
- w_sh_down: bfloat16 [512, 2048], P('tp'), may hold values from -0.25 to 0.25
Outputs:
- mixer_out: bfloat16 [32768, 2048], P(('ep', 'tp'))
- moe_out: bfloat16 [16384, 2048], P(('ep', 'tp'))
The draws below stay inside these ranges and needn't reach their ends.
Inputs may be any that keep to these rules, and one draw needn't show every extreme that they name: `forget_room`: positive and at most 1/6 in every entry. `forget_shift`: constant over each aligned span of 64 positions. `expert_choice`: each row names 4 different experts. In each aligned block of 64 rows no expert is named by more than 6 rows; in every draw one expert is named by exactly 6 rows in every block.
All inputs are finite; a program needn't handle non-finite values.
Results may differ from the reference program's by a relative error of at most 0.02.
Values may be sent and summed in bfloat16 or wider, within the bound.
No kernel may reach another device: no remote copies, remote signals or barrier semaphores. Data moves between devices by JAX's collectives and lax.ppermute only.
A program may use at most 128 MiB of HBM per device.

```python
import jax
import jax.numpy as jnp
from jax import lax

D = 2048
HEADS = 16
HEAD_K = 64
HEAD_V = 64
MIX_K = 1024
MIX_W = 1024
SPAN = 64
MIX_DEV = 512
LENGTH = 32768
TOK_MOE = 16384
QUARTER = 64
EXPERTS = 64
TOP_K = 4
EXP_FF = 1024
SHARED_FF = 512
MEAN_LOAD = 4
CAP = 6
N_EP = 64
N_TP = 4


def draw_forget_room(key, part):
    keys = jax.random.split(key, 2)
    slow_share = 0.5
    is_slow = jax.random.uniform(keys[0], (HEADS,), jnp.float32) < slow_share
    spread = jax.random.uniform(keys[1], (HEADS, HEAD_K), jnp.float32)
    slow_room = jnp.exp(jnp.log(0.3) + spread * (jnp.log(2.0) - jnp.log(0.3))) / LENGTH
    fast_room = jnp.exp(jnp.log(1.0 / 16.0) + spread * (jnp.log(1.0 / 6.0) - jnp.log(1.0 / 16.0)))
    return jnp.where(is_slow[:, None], slow_room, fast_room).reshape(-1).astype(jnp.float32)


def draw_forget_shift(key, part):
    keys = jax.random.split(key, 2)
    device_part = jax.random.uniform(keys[0], (LENGTH // MIX_DEV,), jnp.float32, -1.5, 1.5)
    block_part = jax.random.uniform(keys[1], (LENGTH // SPAN,), jnp.float32, -1.0, 1.0)
    shifted = jnp.repeat(device_part, MIX_DEV) + jnp.repeat(block_part, SPAN)
    return shifted.astype(jnp.float32)


def draw_expert_choice(key, part):
    blocks = TOK_MOE // QUARTER
    half_load = MEAN_LOAD // 2
    keys = jax.random.split(key, 2)
    fullest = jax.random.randint(keys[0], (), 0, EXPERTS)

    def one_block(block_key):
        inner_keys = jax.random.split(block_key, 3)
        expert_ids = jnp.arange(EXPERTS, dtype=jnp.int32)
        ranking = jax.random.randint(inner_keys[0], (EXPERTS,), 0, 1 << 20) * EXPERTS + expert_ids
        ranking = jnp.where(expert_ids == fullest, -1, ranking)
        ordering = jnp.argsort(ranking)
        offsets = jax.random.randint(inner_keys[1], (EXPERTS // 2,), -half_load, half_load + 1)
        offsets = offsets.at[0].set(half_load)
        counts = MEAN_LOAD + jnp.stack([offsets, -offsets], axis=1).reshape(-1)
        labels = jnp.repeat(ordering, counts, total_repeat_length=QUARTER * TOP_K)
        table = labels.reshape(TOP_K, QUARTER).T
        shuffle = jax.random.permutation(inner_keys[2], QUARTER)
        return table[shuffle]
    block_keys = jax.random.split(keys[1], blocks)
    chosen = jax.vmap(one_block)(block_keys)
    return chosen.reshape(blocks * QUARTER, TOP_K).astype(jnp.int32)


def shard_levels(key, dims, cuts, smallest, top_value):
    factor_of = 1.0
    for axis_at, parts in cuts:
        draws = jax.random.uniform(jax.random.fold_in(jax.random.fold_in(key, 6), axis_at), (parts,), jnp.float32, smallest / len(cuts), top_value / len(cuts))
        factor_of = factor_of * jnp.repeat(jnp.exp(draws), dims[axis_at] // parts).reshape((-1,) + (1,) * (len(dims) - 1 - axis_at))
    return factor_of


def centred(rng, shape, scale, most, cuts=(), held_as=jnp.bfloat16):
    loudness = shard_levels(rng, shape, cuts, -0.22, 0.18) if cuts else 1.0
    array = jax.random.normal(rng, shape, jnp.float32) * scale * loudness
    return jnp.minimum(jnp.maximum(array, -most), most).astype(held_as)


def setup_inputs(seed: int = 0) -> dict:
    key_list = jax.random.split(jax.random.key(seed), 20)
    return {
        "mix_in": centred(key_list[0], (LENGTH, D), 1.0, 6.0, ((0, 64),)),
        "forget_shift": draw_forget_shift(jax.random.fold_in(key_list[19], 71), 0),
        "mix_gain": jnp.clip(1.0 + 0.18 * jax.random.normal(key_list[2], (D,), jnp.float32), 0.1, 1.9),
        "w_query": centred(key_list[3], (D, MIX_K), D ** -0.5, 0.125, ((1, 4),)),
        "w_forget": centred(key_list[4], (D, MIX_K), D ** -0.5, 0.125, ((1, 4),)),
        "w_value": centred(key_list[5], (D, MIX_W), D ** -0.5, 0.125, ((1, 4),)),
        "forget_room": draw_forget_room(jax.random.fold_in(key_list[19], 71), 0),
        "head_gain": jnp.clip(1.0 + 0.18 * jax.random.normal(key_list[7], (MIX_W,), jnp.float32), 0.1, 1.9),
        "w_out": centred(key_list[8], (MIX_W, D), MIX_W ** -0.5, 0.1875, ((0, 4),)),
        "moe_in": centred(key_list[9], (TOK_MOE, D), 1.0, 6.0, ((0, 64),)),
        "moe_gain": jnp.clip(1.0 + 0.18 * jax.random.normal(key_list[10], (D,), jnp.float32), 0.1, 1.9),
        "expert_choice": draw_expert_choice(jax.random.fold_in(key_list[19], 71), 0),
        "route_logit": centred(key_list[12], (TOK_MOE, TOP_K), 1.5, 6.0, ((0, 256),), jnp.float32),
        "w_exp_gate": centred(key_list[13], (EXPERTS, D, EXP_FF), D ** -0.5, 0.125, ((0, 64), (2, 4))),
        "w_exp_up": centred(key_list[14], (EXPERTS, D, EXP_FF), D ** -0.5, 0.125, ((0, 64), (2, 4))),
        "w_exp_down": centred(key_list[15], (EXPERTS, EXP_FF, D), EXP_FF ** -0.5, 0.1875, ((0, 64), (1, 4))),
        "w_sh_gate": centred(key_list[16], (D, SHARED_FF), D ** -0.5, 0.125, ((1, 4),)),
        "w_sh_up": centred(key_list[17], (D, SHARED_FF), D ** -0.5, 0.125, ((1, 4),)),
        "w_sh_down": centred(key_list[18], (SHARED_FF, D), SHARED_FF ** -0.5, 0.25, ((0, 4),)),
    }


epsilon = 1e-06
route_scale = 2.5
highest = lax.Precision.HIGHEST

def norm_rows(row_data, gain_vec):
    widened = row_data.astype(jnp.float32)
    scaled = widened * lax.rsqrt(lax.optimization_barrier(jnp.mean(widened * widened, axis=-1, keepdims=True)) + epsilon)
    return (scaled * gain_vec).astype(jnp.bfloat16)

def block_terms(queries, keyed, log_forget, values, span_len):
    token_count, head_count, key_width = queries.shape
    blocks = token_count // span_len
    key_shape = (blocks, span_len, head_count, key_width)
    queries = queries.reshape(key_shape)
    keyed = keyed.reshape(key_shape)
    log_forget = log_forget.reshape(key_shape)
    values = values.reshape(blocks, span_len, head_count, values.shape[-1])
    log_decay = jnp.cumsum(log_forget, axis=1)
    middle = log_decay[:, span_len // 2:span_len // 2 + 1]
    block_end = log_decay[:, span_len - 1:]
    scores = jnp.einsum('nthd,nshd->nhts', queries * jnp.exp(log_decay - middle), keyed * jnp.exp(middle - log_decay), precision=highest)
    causal = jnp.arange(span_len)[:, None] >= jnp.arange(span_len)[None, :]
    scores = jnp.where(causal, scores, 0.0)
    within = jnp.einsum('nhts,nshv->nthv', scores, values, precision=highest)
    query_decay = queries * jnp.exp(log_decay)
    decay_total = jnp.exp(block_end[:, 0])
    state_added = jnp.einsum('nshd,nshv->nhdv', keyed * jnp.exp(block_end - log_decay), values, precision=highest)
    return (within, query_decay, decay_total, state_added)

def split_sum(left, right, groups):
    group_width = left.shape[1] // groups
    running = jnp.zeros((left.shape[0], right.shape[1]), jnp.float32)
    for member in range(groups):
        partial_value = jnp.dot(left[:, member * group_width:(member + 1) * group_width], right[member * group_width:(member + 1) * group_width], preferred_element_type=jnp.float32)
        rounded = lax.optimization_barrier(partial_value.astype(jnp.bfloat16))
        running = running + rounded.astype(jnp.float32)
    return running

def mixer_heads(mix_in, forget_shift, mix_gain, w_query, w_forget, w_value, forget_room, head_gain):
    normed = norm_rows(mix_in, mix_gain)
    queries = jax.nn.silu(jnp.dot(normed, w_query, preferred_element_type=jnp.float32))
    before = jnp.dot(normed, w_forget, preferred_element_type=jnp.float32) + forget_shift[:, None]
    values = jnp.dot(normed, w_value, preferred_element_type=jnp.float32)
    forget_rate = forget_room * jax.nn.sigmoid(-before)
    log_forget = jnp.log1p(-forget_rate)
    token_count = normed.shape[0]
    head_count = values.shape[1] // HEAD_V
    key_shape = (token_count, head_count, HEAD_K)
    within, query_decay, decay_total, state_added = block_terms(queries.reshape(key_shape), forget_rate.reshape(key_shape), log_forget.reshape(key_shape), values.reshape(token_count, head_count, HEAD_V), SPAN)

    def advance(state_now, pieces):
        return (pieces[0][..., None] * state_now + pieces[1], state_now)
    zero_state = jnp.zeros(state_added.shape[1:], jnp.float32)
    state_in = lax.scan(advance, zero_state, (decay_total, state_added))[1]
    mixed = within + jnp.einsum('nthd,nhdv->nthv', query_decay, state_in, precision=highest)
    mixed = mixed.reshape(token_count, head_count, HEAD_V)
    normal = mixed * lax.rsqrt(lax.optimization_barrier(jnp.mean(mixed * mixed, axis=-1, keepdims=True)) + epsilon)
    head_out = (normal * head_gain.reshape(head_count, HEAD_V)).astype(jnp.bfloat16)
    return head_out.reshape(token_count, head_count * HEAD_V)

def experts_out(hidden, expert_choice, weights, w_exp_gate, w_exp_up, w_exp_down):
    token_count = hidden.shape[0]
    slot_limit = N_TP * N_EP * CAP
    flat_ids = expert_choice.reshape(-1)
    flat_tokens = (jnp.arange(flat_ids.shape[0]) // TOP_K).astype(jnp.int32)
    flat_weights = weights.reshape(-1)
    padded = jnp.concatenate([hidden, jnp.zeros((1, hidden.shape[1]), jnp.bfloat16)], axis=0)

    def one_expert(running, pieces):
        expert_index, gate_weight, up_weight, down_weight = pieces
        chosen = flat_ids == expert_index
        places = jnp.where(chosen, jnp.cumsum(chosen.astype(jnp.int32)) - 1, slot_limit).astype(jnp.int32)
        source = jnp.full((slot_limit,), token_count, jnp.int32).at[places].set(flat_tokens, mode='drop')
        slot_weight = jnp.zeros((slot_limit,), jnp.float32).at[places].set(flat_weights, mode='drop')
        gathered = padded[source]
        gate_pre = jnp.dot(gathered, gate_weight, preferred_element_type=jnp.float32)
        up_pre = jnp.dot(gathered, up_weight, preferred_element_type=jnp.float32)
        activations = (jax.nn.silu(gate_pre) * up_pre).astype(jnp.bfloat16)
        outcome = split_sum(activations, down_weight, N_TP).astype(jnp.bfloat16)
        running = running.at[source].add(slot_weight[:, None] * outcome.astype(jnp.float32), mode='drop')
        return (running, None)
    start_sum = jnp.zeros(hidden.shape, jnp.float32)
    expert_ids = jnp.arange(w_exp_gate.shape[0], dtype=jnp.int32)
    return lax.scan(one_expert, start_sum, (expert_ids, w_exp_gate, w_exp_up, w_exp_down))[0]

def reference(mix_in, forget_shift, mix_gain, w_query, w_forget, w_value, forget_room, head_gain, w_out, moe_in, moe_gain, expert_choice, route_logit, w_exp_gate, w_exp_up, w_exp_down, w_sh_gate, w_sh_up, w_sh_down):
    head_out = mixer_heads(mix_in, forget_shift, mix_gain, w_query, w_forget, w_value, forget_room, head_gain)
    mixer_out = split_sum(head_out, w_out, N_TP).astype(jnp.bfloat16)
    hidden = norm_rows(moe_in, moe_gain)
    chance = jax.nn.sigmoid(route_logit)
    weights = chance / lax.optimization_barrier(jnp.sum(chance, axis=-1, keepdims=True)) * route_scale
    routed = experts_out(hidden, expert_choice, weights, w_exp_gate, w_exp_up, w_exp_down)
    shared_gate = jnp.dot(hidden, w_sh_gate, preferred_element_type=jnp.float32)
    shared_up = jnp.dot(hidden, w_sh_up, preferred_element_type=jnp.float32)
    shared_act = (jax.nn.silu(shared_gate) * shared_up).astype(jnp.bfloat16)
    shared_sum = split_sum(shared_act, w_sh_down, N_TP)
    moe_out = (routed + shared_sum).astype(jnp.bfloat16)
    return (mixer_out, moe_out)
```

```python
import jax
import jax.numpy as jnp
from jax import lax
from jax.experimental import pallas as pl
from jax.experimental.pallas import tpu as pltpu
from jax.sharding import Mesh
from jax.sharding import PartitionSpec as P

HEAD = 64
SPAN = 64
TOP_K = 4
EP = ("ep_0", "ep_1", "ep_2")
EP_TP = ("ep_0", "ep_1", "ep_2", "tp")
UP = [(i, (i + 1) % 4) for i in range(4)]
DOWN = [(i, (i - 1) % 4) for i in range(4)]

epsilon = 1e-06
route_scale = 2.5
f32 = jnp.float32
bf16 = jnp.bfloat16


def dot(a, b, ca=1, cb=0, **kw):
    return lax.dot_general(a, b, (((ca,), (cb,)), ((), ())), preferred_element_type=f32, **kw)


def norm_rows(row_data, gain_vec):
    widened = row_data.astype(f32)
    scaled = widened * lax.rsqrt(jnp.mean(widened * widened, axis=-1, keepdims=True) + epsilon)
    return (scaled * gain_vec).astype(bf16)


def same_head(rows, cols):
    row_head = lax.broadcasted_iota(jnp.int32, (rows, cols), 0) // HEAD
    col_head = lax.broadcasted_iota(jnp.int32, (rows, cols), 1) // HEAD
    return row_head == col_head


def mixer_local_body(
    shift_ref, x_hbm, gain_ref, wq_hbm, wf_hbm, wv_hbm, room_ref,
    part_ref, reach_ref, state_ref, total_ref,
    x_ref, wq_ref, wf_ref, wv_ref, normed_ref, q_ref, f_ref, v_ref, sems,
):
    pairs = ((x_hbm, x_ref), (wf_hbm, wf_ref), (wq_hbm, wq_ref), (wv_hbm, wv_ref))
    copies = [pltpu.make_async_copy(a, b, sems.at[i]) for i, (a, b) in enumerate(pairs)]
    for copy in copies:
        copy.start()
    rows, width = q_ref.shape
    blocks = rows // SPAN
    heads = width // HEAD
    gain = gain_ref[...]

    def norm_block(n, carry):
        at = pl.ds(n * SPAN, SPAN)
        normed_ref[at, :] = norm_rows(x_ref[at, :], gain)
        return carry

    copies[0].wait()
    lax.fori_loop(0, blocks, norm_block, 0)
    normed = normed_ref[...]
    copies[1].wait()
    f_ref[...] = dot(normed, wf_ref[...])
    copies[2].wait()
    q_ref[...] = dot(normed, wq_ref[...])
    copies[3].wait()
    v_ref[...] = dot(normed, wv_ref[...])
    room = room_ref[...]
    diagonal = same_head(width, width).astype(f32)
    row_at = lax.broadcasted_iota(jnp.int32, (width, SPAN), 0) % SPAN
    causal = row_at >= lax.broadcasted_iota(jnp.int32, (width, SPAN), 1)
    lower = (
        lax.broadcasted_iota(jnp.int32, (SPAN, SPAN), 0)
        >= lax.broadcasted_iota(jnp.int32, (SPAN, SPAN), 1)
    ).astype(f32)
    state = jnp.zeros((width, width), f32)
    log_before = jnp.zeros((1, width), f32)
    for n in range(blocks):
        at = pl.ds(n * SPAN, SPAN)
        queries = jax.nn.silu(q_ref[at, :])
        rate = room * jax.nn.sigmoid(-(f_ref[at, :] + shift_ref[n]))
        values = v_ref[at, :].astype(bf16)
        log_decay = dot(lower, jnp.log1p(-rate), precision=lax.Precision.HIGHEST)
        middle = log_decay[SPAN // 2 : SPAN // 2 + 1]
        block_end = log_decay[SPAN - 1 :]
        from_middle = queries * jnp.exp(log_decay - middle)
        to_middle = (rate * jnp.exp(middle - log_decay)).astype(bf16)
        by_head = (jnp.concatenate([from_middle] * heads, axis=0) * diagonal).astype(bf16)
        scores = jnp.where(causal, dot(by_head, to_middle, 1, 1), 0.0).astype(bf16)
        all_pairs = dot(scores, values) * diagonal
        mixed = all_pairs[:SPAN]
        for h in range(1, heads):
            mixed = mixed + all_pairs[h * SPAN : (h + 1) * SPAN]
        decayed = queries * jnp.exp(log_decay)
        part_ref[at, :] = mixed + dot(decayed.astype(bf16), state.astype(bf16), 1, 1)
        reach_ref[at, :] = (decayed * jnp.exp(log_before)).astype(bf16)
        to_end = (rate * jnp.exp(block_end - log_decay)).astype(bf16)
        state = state * jnp.exp(block_end) + dot(values, to_end, 0, 0) * diagonal
        log_before = log_before + block_end
    packed = state[:HEAD]
    for h in range(1, heads):
        packed = packed + state[h * HEAD : (h + 1) * HEAD]
    state_ref[...] = packed
    total_ref[...] = jnp.exp(log_before)


def mixer_local(mix_in, shifts, gain, w_query, w_forget, w_value, room):
    rows = mix_in.shape[0]
    width = w_query.shape[1]
    vmem = pl.BlockSpec(memory_space=pltpu.VMEM)
    hbm = pl.BlockSpec(memory_space=pltpu.HBM)
    return pl.pallas_call(
        mixer_local_body,
        in_specs=[pl.BlockSpec(memory_space=pltpu.SMEM), hbm, vmem, hbm, hbm, hbm, vmem],
        out_specs=[vmem] * 4,
        out_shape=[
            jax.ShapeDtypeStruct((rows, width), f32),
            jax.ShapeDtypeStruct((rows, width), bf16),
            jax.ShapeDtypeStruct((HEAD, width), f32),
            jax.ShapeDtypeStruct((1, width), f32),
        ],
        scratch_shapes=[pltpu.VMEM(mix_in.shape, bf16)]
        + [pltpu.VMEM(w_query.shape, bf16)] * 3
        + [pltpu.VMEM(mix_in.shape, bf16)]
        + [pltpu.VMEM((rows, width), f32)] * 3
        + [pltpu.SemaphoreType.DMA((4,))],
        compiler_params=pltpu.CompilerParams(vmem_limit_bytes=60 << 20),
        cost_estimate=pl.CostEstimate(
            flops=rows * mix_in.shape[1] * width * 6, bytes_accessed=6 << 20, transcendentals=0
        ),
        name="mixer_local",
    )(shifts, mix_in, gain, w_query, w_forget, w_value, room)


def state_scan_body(got_ref, out_ref):
    def step(i, state):
        tile = got_ref[i].astype(f32)
        out_ref[i] = state.astype(bf16)
        added = tile[0:2] + tile[2:4]
        decay = tile[4:6] + tile[6:8]
        return decay * state + added

    lax.fori_loop(0, got_ref.shape[0], step, jnp.zeros((2, 128), f32), unroll=8)


def state_scan(got):
    return pl.pallas_call(
        state_scan_body,
        out_shape=jax.ShapeDtypeStruct((got.shape[0], 2, 128), bf16),
        name="state_scan",
    )(got)


def split_bf16(x):
    high = x.astype(bf16)
    return high, (x - high.astype(f32)).astype(bf16)


def mixer_out_body(rank_ref, part_ref, reach_ref, state_ref, gain_ref, w_ref, out_ref):
    width = part_ref.shape[1]
    heads = width // HEAD
    diagonal = same_head(width, width).astype(f32)
    state = jnp.concatenate([state_ref[...].astype(f32)] * heads, axis=0) * diagonal
    mixed = part_ref[...] + dot(reach_ref[...], state.astype(bf16), 1, 1)
    square = dot(mixed * mixed, diagonal * (1.0 / HEAD), precision=lax.Precision.HIGHEST)
    head_out = (mixed * lax.rsqrt(square + epsilon) * gain_ref[...]).astype(bf16)
    out_ref[0] = dot(head_out, w_ref[...]).astype(bf16)


def mixer_out(rank, part, reach, state, gain, w_out, tp_count):
    rows, width = part.shape
    quarter = rows // tp_count
    model = w_out.shape[1]
    mine = lambda i, rank: ((rank[0] + i) % tp_count, 0)
    whole = lambda i, rank: (0, 0)
    return pl.pallas_call(
        mixer_out_body,
        grid_spec=pltpu.PrefetchScalarGridSpec(
            num_scalar_prefetch=1,
            grid=(tp_count,),
            in_specs=[
                pl.BlockSpec((quarter, width), mine),
                pl.BlockSpec((quarter, width), mine),
                pl.BlockSpec((HEAD, width), whole),
                pl.BlockSpec((1, width), whole),
                pl.BlockSpec((width, model), whole),
            ],
            out_specs=pl.BlockSpec((1, quarter, model), lambda i, rank: (i, 0, 0)),
        ),
        out_shape=jax.ShapeDtypeStruct((tp_count, quarter, model), bf16),
        cost_estimate=pl.CostEstimate(
            flops=rows * width * model * 2, bytes_accessed=4 << 20, transcendentals=0
        ),
        name="mixer_out",
    )(rank, part, reach, state, gain, w_out)


def hidden_units_body(x_ref, gate_ref, up_ref, out_ref, gate_sum, up_sum):
    step = pl.program_id(0)

    @pl.when(step == 0)
    def _():
        gate_sum[...] = jnp.zeros(gate_sum.shape, f32)
        up_sum[...] = jnp.zeros(up_sum.shape, f32)

    x = x_ref[...]
    gate_sum[...] += dot(x, gate_ref[...])
    up_sum[...] += dot(x, up_ref[...])

    @pl.when(step == pl.num_programs(0) - 1)
    def _():
        out_ref[...] = (jax.nn.silu(gate_sum[...]) * up_sum[...]).astype(bf16)


def hidden_units(x, gate, up):
    rows, model = x.shape
    width = gate.shape[1]
    part = model // 4
    return pl.pallas_call(
        hidden_units_body,
        grid=(model // part,),
        in_specs=[
            pl.BlockSpec((rows, part), lambda i: (0, i)),
            pl.BlockSpec((part, width), lambda i: (i, 0)),
            pl.BlockSpec((part, width), lambda i: (i, 0)),
        ],
        out_specs=pl.BlockSpec((rows, width), lambda i: (0, 0)),
        out_shape=jax.ShapeDtypeStruct((rows, width), bf16),
        scratch_shapes=[pltpu.VMEM((rows, width), f32)] * 2,
        cost_estimate=pl.CostEstimate(
            flops=rows * model * width * 4, bytes_accessed=4 << 20, transcendentals=0
        ),
        name="hidden_units",
    )(x, gate, up)


def shift_up(x):
    return lax.ppermute(x, "tp", UP)


def shift_down(x):
    return lax.ppermute(x, "tp", DOWN)


def after(x, *others):
    return lax.optimization_barrier((x, *others))[0]


def local(
    mix_in,
    forget_shift,
    mix_gain,
    w_query,
    w_forget,
    w_value,
    forget_room,
    head_gain,
    w_out,
    moe_in,
    moe_gain,
    expert_choice,
    route_logit,
    w_exp_gate,
    w_exp_up,
    w_exp_down,
    w_sh_gate,
    w_sh_up,
    w_sh_down,
):
    tp_count = 4
    tp_rank = lax.axis_index("tp")
    row_count, model = moe_in.shape
    quarter = row_count // tp_count
    experts = lax.axis_size(EP) * w_exp_gate.shape[0]
    mean_load = quarter * TOP_K // experts
    capacity = mean_load + mean_load // 2
    slots = experts * capacity
    pieces = capacity * model // 128

    gate_own, up_own, down_own = w_exp_gate[0], w_exp_up[0], w_exp_down[0]
    gate_below = shift_up(gate_own)
    up_above = shift_down(up_own)
    up_below = shift_up(up_own)
    gate_above = shift_down(gate_own)
    gate_far = shift_up(gate_below)
    up_far = shift_down(up_above)
    half_units = down_own.shape[0] // 2
    top, low = down_own[:half_units], down_own[half_units:]
    top_below = shift_up(top)
    low_above = shift_down(low)
    low_below = shift_up(low)
    top_above = shift_down(top)

    shifts = forget_shift.reshape(-1, SPAN)[:, 0]
    part, reach, added, total = mixer_local(
        mix_in, shifts, mix_gain[None], w_query, w_forget, w_value, forget_room[None]
    )
    added_high, added_low = split_bf16(added)
    total_high, total_low = split_bf16(total)
    whole_row = lambda x: jnp.broadcast_to(x.reshape(1, 2, 128), (HEAD, 2, 128))
    state_send = [
        added_high.reshape(HEAD, 2, 128),
        added_low.reshape(HEAD, 2, 128),
        whole_row(total_high),
        whole_row(total_low),
    ]

    moe_in, expert_choice = lax.optimization_barrier((moe_in, expert_choice, total))[:2]
    own_rows = lax.dynamic_slice_in_dim(moe_in, tp_rank * quarter, quarter, 0)
    own_hidden = norm_rows(own_rows, moe_gain)
    labels = lax.dynamic_slice_in_dim(expert_choice, tp_rank * quarter, quarter, 0).reshape(-1)
    onehot = labels[:, None] == jnp.arange(experts, dtype=jnp.int32)[None, :]
    earlier = jnp.arange(labels.shape[0])[:, None] > jnp.arange(labels.shape[0])[None, :]
    counts = dot(earlier.astype(bf16), onehot.astype(bf16))
    places = jnp.sum(jnp.where(onehot, counts, 0.0), axis=-1).astype(jnp.int32)
    slot_ids = (labels * capacity + places).reshape(quarter, TOP_K)
    slot_axis = jnp.arange(slots, dtype=jnp.int32)
    holds = sum((slot_ids[:, k][None, :] == slot_axis[:, None]).astype(bf16) for k in range(TOP_K))
    outgoing = dot(holds, own_hidden).astype(bf16)
    arrived = lax.all_to_all(
        jnp.concatenate([outgoing.reshape(experts, pieces, 128)] + state_send, axis=1),
        EP, split_axis=0, concat_axis=0, tiled=True,
    )
    state_next = state_scan(arrived[:, pieces:])
    top_far = shift_up(after(top_below, state_next))
    low_far = shift_down(after(low_above, state_next))
    state_start = lax.all_to_all(
        state_next, EP, split_axis=0, concat_axis=0, tiled=True
    ).reshape(HEAD, -1)
    mixer_parts = mixer_out(
        tp_rank.reshape(1), part, reach, state_start, head_gain[None], w_out, tp_count
    )

    hidden = norm_rows(moe_in, moe_gain)
    shared_gate = dot(hidden, w_sh_gate)
    shared_up = dot(hidden, w_sh_up)
    shared_act = (jax.nn.silu(shared_gate) * shared_up).astype(bf16)
    shared_part = dot(shared_act, w_sh_down).astype(bf16)
    chunk = lambda i: jnp.concatenate(
        [
            mixer_parts[i],
            lax.dynamic_slice_in_dim(shared_part, ((tp_rank + i) % tp_count) * quarter, quarter, 0),
        ],
        axis=0,
    )

    x = arrived[:, :pieces].reshape(slots, model)
    acts = [
        hidden_units(x, gate_own, up_own),
        hidden_units(x, gate_below, up_below),
        hidden_units(x, gate_above, up_above),
        hidden_units(x, gate_far, up_far),
    ]
    down = [(top, low), (top_below, low_below), (top_above, low_above), (top_far, low_far)]
    weights = jax.nn.sigmoid(route_logit)
    weights = weights / jnp.sum(weights, axis=-1, keepdims=True) * route_scale
    choose = sum(
        jnp.where(slot_ids[:, k][:, None] == slot_axis[None, :], weights[:, k][:, None], 0.0)
        for k in range(TOP_K)
    )
    choose_high, choose_low = split_bf16(choose)
    summed = sum(
        (dot(a[:, :half_units], top) + dot(a[:, half_units:], low)).astype(bf16).astype(f32)
        for a, (top, low) in zip(acts, down)
    )
    returned = lax.all_to_all(
        summed.astype(bf16).reshape(experts, pieces, 128),
        EP, split_axis=0, concat_axis=0, tiled=True,
    ).reshape(slots, model)
    routed = dot(choose_high, returned) + dot(choose_low, returned)

    across = chunk(2)
    middle = across.shape[0] // 2
    via_below = shift_up(across[:middle])
    via_above = shift_down(across[middle:])
    to_above = chunk(1)
    to_above = jnp.concatenate([to_above[:middle] + via_below, to_above[middle:]], axis=0)
    to_below = chunk(3)
    to_below = jnp.concatenate([to_below[:middle], to_below[middle:] + via_above], axis=0)
    from_below = shift_up(to_above)
    from_above = shift_down(to_below)
    total_rows = chunk(0).astype(f32) + from_below.astype(f32) + from_above.astype(f32)
    mixer_rows = mix_in.shape[0] // tp_count
    return (
        total_rows[:mixer_rows].astype(bf16),
        (routed + total_rows[mixer_rows:]).astype(bf16),
    )


def solution(mesh):
    finer = Mesh(mesh.devices.reshape(8, 4, 2, mesh.shape["tp"]), ("ep_0", "ep_1", "ep_2", "tp"))
    in_specs = (
        P(EP, None),
        P(EP),
        P(),
        P(None, "tp"),
        P(None, "tp"),
        P(None, "tp"),
        P("tp"),
        P("tp"),
        P("tp", None),
        P(EP, None),
        P(),
        P(EP, None),
        P(EP_TP, None),
        P(EP, None, "tp"),
        P(EP, None, "tp"),
        P(EP, "tp", None),
        P(None, "tp"),
        P(None, "tp"),
        P("tp", None),
    )
    out_specs = (P(EP_TP, None), P(EP_TP, None))

    return jax.shard_map(local, mesh=finer, in_specs=in_specs, out_specs=out_specs, check_vma=False)
```

```python
import jax
import jax.numpy as jnp
from jax import lax
from jax.experimental import pallas as pl
from jax.experimental.pallas import tpu as pltpu
from jax.sharding import Mesh
from jax.sharding import PartitionSpec as P

HEAD = 64
SPAN = 64
TOP_K = 4
EP = ("ep_0", "ep_1", "ep_2")
EP_TP = ("ep_0", "ep_1", "ep_2", "tp")
UP = [(i, (i + 1) % 4) for i in range(4)]
DOWN = [(i, (i - 1) % 4) for i in range(4)]

epsilon = 1e-06
route_scale = 2.5
f32 = jnp.float32
bf16 = jnp.bfloat16


def dot(a, b, ca=1, cb=0, **kw):
    return lax.dot_general(a, b, (((ca,), (cb,)), ((), ())), preferred_element_type=f32, **kw)


def norm_rows(row_data, gain_vec):
    widened = row_data.astype(f32)
    scaled = widened * lax.rsqrt(jnp.mean(widened * widened, axis=-1, keepdims=True) + epsilon)
    return (scaled * gain_vec).astype(bf16)


def same_head(rows, cols):
    row_head = lax.broadcasted_iota(jnp.int32, (rows, cols), 0) // HEAD
    col_head = lax.broadcasted_iota(jnp.int32, (rows, cols), 1) // HEAD
    return row_head == col_head


def mixer_local_body(
    shift_ref, x_hbm, gain_ref, wq_hbm, wf_hbm, wv_hbm, room_ref,
    part_ref, reach_ref, state_ref, total_ref,
    x_ref, wq_ref, wf_ref, wv_ref, normed_ref, q_ref, f_ref, v_ref, sems,
):
    pairs = ((x_hbm, x_ref), (wf_hbm, wf_ref), (wq_hbm, wq_ref), (wv_hbm, wv_ref))
    copies = [pltpu.make_async_copy(a, b, sems.at[i]) for i, (a, b) in enumerate(pairs)]
    for copy in copies:
        copy.start()
    rows, width = q_ref.shape
    blocks = rows // SPAN
    heads = width // HEAD
    gain = gain_ref[...]

    def norm_block(n, carry):
        at = pl.ds(n * SPAN, SPAN)
        normed_ref[at, :] = norm_rows(x_ref[at, :], gain)
        return carry

    copies[0].wait()
    lax.fori_loop(0, blocks, norm_block, 0)
    normed = normed_ref[...]
    copies[1].wait()
    f_ref[...] = dot(normed, wf_ref[...])
    copies[2].wait()
    q_ref[...] = dot(normed, wq_ref[...])
    copies[3].wait()
    v_ref[...] = dot(normed, wv_ref[...])
    room = room_ref[...]
    diagonal = same_head(width, width).astype(f32)
    row_at = lax.broadcasted_iota(jnp.int32, (width, SPAN), 0) % SPAN
    causal = row_at >= lax.broadcasted_iota(jnp.int32, (width, SPAN), 1)
    lower = (
        lax.broadcasted_iota(jnp.int32, (SPAN, SPAN), 0)
        >= lax.broadcasted_iota(jnp.int32, (SPAN, SPAN), 1)
    ).astype(f32)
    state = jnp.zeros((width, width), f32)
    log_before = jnp.zeros((1, width), f32)
    for n in range(blocks):
        at = pl.ds(n * SPAN, SPAN)
        queries = jax.nn.silu(q_ref[at, :])
        rate = room * jax.nn.sigmoid(-(f_ref[at, :] + shift_ref[n]))
        values = v_ref[at, :].astype(bf16)
        log_decay = dot(lower, jnp.log1p(-rate), precision=lax.Precision.HIGHEST)
        middle = log_decay[SPAN // 2 : SPAN // 2 + 1]
        block_end = log_decay[SPAN - 1 :]
        from_middle = queries * jnp.exp(log_decay - middle)
        to_middle = (rate * jnp.exp(middle - log_decay)).astype(bf16)
        by_head = (jnp.concatenate([from_middle] * heads, axis=0) * diagonal).astype(bf16)
        scores = jnp.where(causal, dot(by_head, to_middle, 1, 1), 0.0).astype(bf16)
        all_pairs = dot(scores, values) * diagonal
        mixed = all_pairs[:SPAN]
        for h in range(1, heads):
            mixed = mixed + all_pairs[h * SPAN : (h + 1) * SPAN]
        decayed = queries * jnp.exp(log_decay)
        part_ref[at, :] = mixed + dot(decayed.astype(bf16), state.astype(bf16), 1, 1)
        reach_ref[at, :] = (decayed * jnp.exp(log_before)).astype(bf16)
        to_end = (rate * jnp.exp(block_end - log_decay)).astype(bf16)
        state = state * jnp.exp(block_end) + dot(values, to_end, 0, 0) * diagonal
        log_before = log_before + block_end
    packed = state[:HEAD]
    for h in range(1, heads):
        packed = packed + state[h * HEAD : (h + 1) * HEAD]
    state_ref[...] = packed
    total_ref[...] = jnp.exp(log_before)


def mixer_local(mix_in, shifts, gain, w_query, w_forget, w_value, room):
    rows = mix_in.shape[0]
    width = w_query.shape[1]
    vmem = pl.BlockSpec(memory_space=pltpu.VMEM)
    hbm = pl.BlockSpec(memory_space=pltpu.HBM)
    return pl.pallas_call(
        mixer_local_body,
        in_specs=[pl.BlockSpec(memory_space=pltpu.SMEM), hbm, vmem, hbm, hbm, hbm, vmem],
        out_specs=[vmem] * 4,
        out_shape=[
            jax.ShapeDtypeStruct((rows, width), f32),
            jax.ShapeDtypeStruct((rows, width), bf16),
            jax.ShapeDtypeStruct((HEAD, width), f32),
            jax.ShapeDtypeStruct((1, width), f32),
        ],
        scratch_shapes=[pltpu.VMEM(mix_in.shape, bf16)]
        + [pltpu.VMEM(w_query.shape, bf16)] * 3
        + [pltpu.VMEM(mix_in.shape, bf16)]
        + [pltpu.VMEM((rows, width), f32)] * 3
        + [pltpu.SemaphoreType.DMA((4,))],
        compiler_params=pltpu.CompilerParams(vmem_limit_bytes=60 << 20),
        cost_estimate=pl.CostEstimate(
            flops=rows * mix_in.shape[1] * width * 6, bytes_accessed=6 << 20, transcendentals=0
        ),
        name="mixer_local",
    )(shifts, mix_in, gain, w_query, w_forget, w_value, room)


def state_scan_body(got_ref, out_ref):
    def step(i, state):
        tile = got_ref[i].astype(f32)
        out_ref[i] = state.astype(bf16)
        added = tile[0:2] + tile[2:4]
        decay = tile[4:6] + tile[6:8]
        return decay * state + added

    lax.fori_loop(0, got_ref.shape[0], step, jnp.zeros((2, 128), f32), unroll=8)


def state_scan(arrived, pieces):
    peers = arrived.shape[0]
    return pl.pallas_call(
        state_scan_body,
        grid=(1,),
        in_specs=[pl.BlockSpec((peers, 8, 128), lambda i: (0, pieces // 8, 0))],
        out_specs=pl.BlockSpec((peers, 2, 128), lambda i: (0, 0, 0)),
        out_shape=jax.ShapeDtypeStruct((peers, 2, 128), bf16),
        compiler_params=pltpu.CompilerParams(vmem_limit_bytes=60 << 20),
        name="state_scan",
    )(arrived)


def split_bf16(x):
    high = x.astype(bf16)
    return high, (x - high.astype(f32)).astype(bf16)


def mixer_out_body(rank_ref, part_ref, reach_ref, state_ref, gain_ref, w_ref, out_ref):
    width = part_ref.shape[1]
    heads = width // HEAD
    diagonal = same_head(width, width).astype(f32)
    state = jnp.concatenate([state_ref[...].astype(f32)] * heads, axis=0) * diagonal
    mixed = part_ref[...] + dot(reach_ref[...], state.astype(bf16), 1, 1)
    square = dot(mixed * mixed, diagonal * (1.0 / HEAD), precision=lax.Precision.HIGHEST)
    head_out = (mixed * lax.rsqrt(square + epsilon) * gain_ref[...]).astype(bf16)
    out_ref[0] = dot(head_out, w_ref[...]).astype(bf16)


def mixer_out(rank, part, reach, state, gain, w_out, tp_count):
    rows, width = part.shape
    quarter = rows // tp_count
    model = w_out.shape[1]
    mine = lambda i, rank: ((rank[0] + i) % tp_count, 0)
    whole = lambda i, rank: (0, 0)
    return pl.pallas_call(
        mixer_out_body,
        grid_spec=pltpu.PrefetchScalarGridSpec(
            num_scalar_prefetch=1,
            grid=(tp_count,),
            in_specs=[
                pl.BlockSpec((quarter, width), mine),
                pl.BlockSpec((quarter, width), mine),
                pl.BlockSpec((HEAD, width), whole),
                pl.BlockSpec((1, width), whole),
                pl.BlockSpec((width, model), whole),
            ],
            out_specs=pl.BlockSpec((1, quarter, model), lambda i, rank: (i, 0, 0)),
        ),
        out_shape=jax.ShapeDtypeStruct((tp_count, quarter, model), bf16),
        cost_estimate=pl.CostEstimate(
            flops=rows * width * model * 2, bytes_accessed=4 << 20, transcendentals=0
        ),
        name="mixer_out",
    )(rank, part, reach, state, gain, w_out)


def dispatch_body(
    rank_ref, x_ref, choice_ref, gain_ref, state_ref, total_ref, out_ref, slot_ref, rows_ref
):
    quarter, model = x_ref.shape
    experts, stride, _ = out_ref.shape
    capacity = (stride - 8) * 128 // model
    per_row = model // 128
    hidden = norm_rows(x_ref[...], gain_ref[...])
    expert_at = lax.broadcasted_iota(jnp.int32, (quarter, experts), 1)
    chosen = [choice_ref[:, k : k + 1] == expert_at for k in range(TOP_K)]
    named = sum(one.astype(f32) for one in chosen)
    earlier = lax.broadcasted_iota(jnp.int32, (quarter, quarter), 0) > lax.broadcasted_iota(
        jnp.int32, (quarter, quarter), 1
    )
    ranks = dot(earlier.astype(bf16), named.astype(bf16))
    for k in range(TOP_K):
        place = jnp.sum(jnp.where(chosen[k], ranks, 0.0), axis=-1, keepdims=True)
        slot_ref[:, k : k + 1] = choice_ref[:, k : k + 1] * capacity + place.astype(jnp.int32)
    for c in range(capacity):
        holds = jnp.where(ranks == c, named, 0.0).astype(bf16)
        rows = dot(holds, hidden, 0, 0)
        for k in range(per_row):
            rows_ref[pl.ds(c * per_row + k, experts, stride=stride), :] = rows[
                :, k * 128 : (k + 1) * 128
            ]
    base = stride - 8
    state_high = state_ref[...].astype(bf16).astype(f32)
    total = jnp.broadcast_to(total_ref[...], state_ref.shape)
    total_high = total.astype(bf16).astype(f32)
    sent = (state_high, state_ref[...] - state_high, total_high, total - total_high)
    for i, part in enumerate(sent):
        for j in range(2):
            rows_ref[pl.ds(base + 2 * i + j, experts, stride=stride), :] = part[
                :, j * 128 : (j + 1) * 128
            ]

    def narrow(e, carry):
        at = pl.multiple_of(e * stride, 8)
        out_ref[e] = rows_ref[pl.ds(at, stride), :].astype(bf16)
        return carry

    lax.fori_loop(0, experts, narrow, 0)


def dispatch(rank, moe_in, choice, gain, state, total, quarter, experts, pieces):
    model = moe_in.shape[1]
    mine = lambda i, rank: (rank[0], 0)
    whole = lambda i, rank: (0, 0)
    return pl.pallas_call(
        dispatch_body,
        grid_spec=pltpu.PrefetchScalarGridSpec(
            num_scalar_prefetch=1,
            grid=(1,),
            in_specs=[
                pl.BlockSpec((quarter, model), mine),
                pl.BlockSpec((quarter, TOP_K), mine),
                pl.BlockSpec((1, model), whole),
                pl.BlockSpec(state.shape, whole),
                pl.BlockSpec(total.shape, whole),
            ],
            out_specs=[
                pl.BlockSpec((experts, pieces + 8, 128), lambda i, rank: (0, 0, 0)),
                pl.BlockSpec((quarter, TOP_K), whole),
            ],
            scratch_shapes=[pltpu.VMEM((experts * (pieces + 8), 128), f32)],
        ),
        out_shape=[
            jax.ShapeDtypeStruct((experts, pieces + 8, 128), bf16),
            jax.ShapeDtypeStruct((quarter, TOP_K), jnp.int32),
        ],
        name="dispatch",
    )(rank, moe_in, choice, gain, state, total)


def hidden_units_body(got_ref, *refs):
    groups = (len(refs) - 4) // 2
    gates, ups = refs[:groups], refs[groups : 2 * groups]
    out_ref, rows_ref, x_ref, sums_ref = refs[2 * groups :]
    step = pl.program_id(0)
    peers, pieces, _ = got_ref.shape
    steps, slots, part = x_ref.shape
    capacity = slots // peers
    per_row = pieces // capacity

    @pl.when(step == 0)
    def _():
        def widen(e, carry):
            at = pl.multiple_of(e * pieces, 8)
            rows_ref[pl.ds(at, pieces), :] = got_ref[e].astype(f32)
            return carry

        lax.fori_loop(0, peers, widen, 0)
        for c in range(capacity):
            for k in range(per_row):
                column = k * 128 % part
                x_ref[k * 128 // part, c * peers : (c + 1) * peers, column : column + 128] = (
                    rows_ref[pl.ds(c * per_row + k, peers, stride=pieces), :].astype(bf16)
                )
        sums_ref[...] = jnp.zeros(sums_ref.shape, f32)

    x = x_ref[step]
    for i, ref in enumerate(gates + ups):
        sums_ref[i] += dot(x, ref[...])

    @pl.when(step == steps - 1)
    def _():
        for i in range(groups):
            out_ref[i] = (jax.nn.silu(sums_ref[i]) * sums_ref[groups + i]).astype(bf16)


def hidden_units(arrived, gates, ups, pieces):
    peers = arrived.shape[0]
    model, width = gates[0].shape
    slots = peers * pieces * 128 // model
    steps = 4
    part = model // steps
    groups = len(gates)
    weight = pl.BlockSpec((part, width), lambda i: (i, 0))
    return pl.pallas_call(
        hidden_units_body,
        grid=(steps,),
        in_specs=[pl.BlockSpec((peers, pieces, 128), lambda i: (0, 0, 0))]
        + [weight] * (2 * groups),
        out_specs=pl.BlockSpec((groups, slots, width), lambda i: (0, 0, 0)),
        out_shape=jax.ShapeDtypeStruct((groups, slots, width), bf16),
        scratch_shapes=[
            pltpu.VMEM((peers * pieces, 128), f32),
            pltpu.VMEM((steps, slots, part), bf16),
            pltpu.VMEM((2 * groups, slots, width), f32),
        ],
        compiler_params=pltpu.CompilerParams(vmem_limit_bytes=60 << 20),
        cost_estimate=pl.CostEstimate(
            flops=slots * model * width * 4 * groups,
            bytes_accessed=10 << 20,
            transcendentals=0,
        ),
        name="hidden_units",
    )(arrived, *gates, *ups)


def results_body(act_ref, *refs):
    groups = act_ref.shape[0]
    halves = refs[: 2 * groups]
    out_ref, weight_ref, sum_ref, rows_ref, sems = refs[2 * groups :]
    half = halves[0].shape[0]
    copies = []
    for i, ref in enumerate(halves):
        at = pl.ds(i % 2 * half, half)
        copies.append(pltpu.make_async_copy(ref, weight_ref.at[i // 2, at], sems.at[i]))
        copies[-1].start()
    slots, model = sum_ref.shape
    peers, pieces, _ = out_ref.shape
    capacity = slots // peers
    per_row = model // 128
    part = 256
    for g in range(groups):
        copies[2 * g].wait()
        copies[2 * g + 1].wait()
        act = act_ref[g]
        for col in range(0, model, part):
            cols = slice(col, col + part)
            one = dot(act, weight_ref[g, :, cols]).astype(bf16).astype(f32)
            if g == 0:
                sum_ref[:, cols] = one
            elif g < groups - 1:
                sum_ref[:, cols] += one
            else:
                whole = sum_ref[:, cols] + one
                for c in range(capacity):
                    for j in range(part // 128):
                        k = col // 128 + j
                        rows_ref[pl.ds(c * per_row + k, peers, stride=pieces), :] = whole[
                            c * peers : (c + 1) * peers, j * 128 : (j + 1) * 128
                        ]

    def narrow(e, carry):
        at = pl.multiple_of(e * pieces, 8)
        out_ref[e] = rows_ref[pl.ds(at, pieces), :].astype(bf16)
        return carry

    lax.fori_loop(0, peers, narrow, 0)


def results(acts, halves, peers):
    groups, slots, width = acts.shape
    model = halves[0].shape[1]
    pieces = slots // peers * model // 128
    hbm = pl.BlockSpec(memory_space=pltpu.HBM)
    vmem = pl.BlockSpec(memory_space=pltpu.VMEM)
    return pl.pallas_call(
        results_body,
        in_specs=[vmem] + [hbm] * len(halves),
        out_specs=vmem,
        out_shape=jax.ShapeDtypeStruct((peers, pieces, 128), bf16),
        scratch_shapes=[
            pltpu.VMEM((groups, width, model), bf16),
            pltpu.VMEM((slots, model), f32),
            pltpu.VMEM((peers * pieces, 128), f32),
            pltpu.SemaphoreType.DMA((len(halves),)),
        ],
        compiler_params=pltpu.CompilerParams(vmem_limit_bytes=60 << 20),
        cost_estimate=pl.CostEstimate(
            flops=slots * model * width * 2 * groups, bytes_accessed=6 << 20, transcendentals=0
        ),
        name="results",
    )(acts, *halves)


def shift_up(x):
    return lax.ppermute(x, "tp", UP)


def shift_down(x):
    return lax.ppermute(x, "tp", DOWN)


def after(x, *others):
    return lax.optimization_barrier((x, *others))[0]


def local(
    mix_in,
    forget_shift,
    mix_gain,
    w_query,
    w_forget,
    w_value,
    forget_room,
    head_gain,
    w_out,
    moe_in,
    moe_gain,
    expert_choice,
    route_logit,
    w_exp_gate,
    w_exp_up,
    w_exp_down,
    w_sh_gate,
    w_sh_up,
    w_sh_down,
):
    tp_count = 4
    tp_rank = lax.axis_index("tp")
    row_count, model = moe_in.shape
    quarter = row_count // tp_count
    experts = lax.axis_size(EP) * w_exp_gate.shape[0]
    mean_load = quarter * TOP_K // experts
    capacity = mean_load + mean_load // 2
    slots = experts * capacity
    pieces = capacity * model // 128

    gate_own, up_own, down_own = w_exp_gate[0], w_exp_up[0], w_exp_down[0]
    gate_below = shift_up(gate_own)
    up_above = shift_down(up_own)
    up_below = shift_up(up_own)
    gate_above = shift_down(gate_own)
    gate_far = shift_up(gate_below)
    up_far = shift_down(up_above)
    half_units = down_own.shape[0] // 2
    top, low = down_own[:half_units], down_own[half_units:]
    top_below = shift_up(top)
    low_above = shift_down(low)
    low_below = shift_up(low)
    top_above = shift_down(top)

    shifts = forget_shift.reshape(-1, SPAN)[:, 0]
    part, reach, added, total = mixer_local(
        mix_in, shifts, mix_gain[None], w_query, w_forget, w_value, forget_room[None]
    )
    outgoing, slot_ids = dispatch(
        tp_rank.reshape(1), moe_in, expert_choice, moe_gain[None], added, total,
        quarter, experts, pieces,
    )
    arrived = lax.all_to_all(outgoing, EP, split_axis=0, concat_axis=0, tiled=True)
    state_next = state_scan(arrived, pieces)
    top_far = shift_up(after(top_below, state_next))
    low_far = shift_down(after(low_above, state_next))
    state_start = lax.all_to_all(
        state_next, EP, split_axis=0, concat_axis=0, tiled=True
    ).reshape(HEAD, -1)
    mixer_parts = mixer_out(
        tp_rank.reshape(1), part, reach, state_start, head_gain[None], w_out, tp_count
    )

    hidden = norm_rows(moe_in, moe_gain)
    shared_gate = dot(hidden, w_sh_gate)
    shared_up = dot(hidden, w_sh_up)
    shared_act = (jax.nn.silu(shared_gate) * shared_up).astype(bf16)
    shared_part = dot(shared_act, w_sh_down).astype(bf16)
    chunk = lambda i: jnp.concatenate(
        [
            mixer_parts[i],
            lax.dynamic_slice_in_dim(shared_part, ((tp_rank + i) % tp_count) * quarter, quarter, 0),
        ],
        axis=0,
    )

    acts = hidden_units(
        arrived,
        [gate_own, gate_below, gate_above, gate_far],
        [up_own, up_below, up_above, up_far],
        pieces,
    )
    slot_axis = jnp.arange(slots, dtype=jnp.int32)
    weights = jax.nn.sigmoid(route_logit)
    weights = weights / jnp.sum(weights, axis=-1, keepdims=True) * route_scale
    choose = sum(
        jnp.where(slot_ids[:, k][:, None] == slot_axis[None, :], weights[:, k][:, None], 0.0)
        for k in range(TOP_K)
    )
    choose_high, choose_low = split_bf16(choose)
    ready = results(
        acts,
        [top, low, top_below, low_below, top_above, low_above, top_far, low_far],
        experts,
    )
    returned = lax.all_to_all(ready, EP, split_axis=0, concat_axis=0, tiled=True)
    returned = returned.reshape(slots, model)
    routed = dot(choose_high, returned) + dot(choose_low, returned)

    across = chunk(2)
    middle = across.shape[0] // 2
    via_below = shift_up(across[:middle])
    via_above = shift_down(across[middle:])
    to_above = chunk(1)
    to_above = jnp.concatenate([to_above[:middle] + via_below, to_above[middle:]], axis=0)
    to_below = chunk(3)
    to_below = jnp.concatenate([to_below[:middle], to_below[middle:] + via_above], axis=0)
    from_below = shift_up(to_above)
    from_above = shift_down(to_below)
    total_rows = chunk(0).astype(f32) + from_below.astype(f32) + from_above.astype(f32)
    mixer_rows = mix_in.shape[0] // tp_count
    return (
        total_rows[:mixer_rows].astype(bf16),
        (routed + total_rows[mixer_rows:]).astype(bf16),
    )


def solution(mesh):
    finer = Mesh(mesh.devices.reshape(8, 4, 2, mesh.shape["tp"]), ("ep_0", "ep_1", "ep_2", "tp"))
    in_specs = (
        P(EP, None),
        P(EP),
        P(),
        P(None, "tp"),
        P(None, "tp"),
        P(None, "tp"),
        P("tp"),
        P("tp"),
        P("tp", None),
        P(EP, None),
        P(),
        P(EP, None),
        P(EP_TP, None),
        P(EP, None, "tp"),
        P(EP, None, "tp"),
        P(EP, "tp", None),
        P(None, "tp"),
        P(None, "tp"),
        P("tp", None),
    )
    out_specs = (P(EP_TP, None), P(EP_TP, None))

    return jax.shard_map(local, mesh=finer, in_specs=in_specs, out_specs=out_specs, check_vma=False)
```

```python
import jax
import jax.numpy as jnp
from jax import lax
from jax.experimental import pallas as pl
from jax.experimental.pallas import tpu as pltpu
from jax.sharding import Mesh
from jax.sharding import PartitionSpec as P

HEAD = 64
SPAN = 64
TOP_K = 4
EP = ("ep_0", "ep_1", "ep_2")
EP_TP = ("ep_0", "ep_1", "ep_2", "tp")
UP = [(i, (i + 1) % 4) for i in range(4)]
DOWN = [(i, (i - 1) % 4) for i in range(4)]

epsilon = 1e-06
route_scale = 2.5
f32 = jnp.float32
bf16 = jnp.bfloat16


def dot(a, b, ca=1, cb=0, **kw):
    return lax.dot_general(a, b, (((ca,), (cb,)), ((), ())), preferred_element_type=f32, **kw)


def norm_rows(row_data, gain_vec):
    widened = row_data.astype(f32)
    scaled = widened * lax.rsqrt(jnp.mean(widened * widened, axis=-1, keepdims=True) + epsilon)
    return (scaled * gain_vec).astype(bf16)


def same_head(rows, cols):
    row_head = lax.broadcasted_iota(jnp.int32, (rows, cols), 0) // HEAD
    col_head = lax.broadcasted_iota(jnp.int32, (rows, cols), 1) // HEAD
    return row_head == col_head


def mixer_local_body(
    shift_ref, x_hbm, gain_ref, wq_hbm, wf_hbm, wv_hbm, room_ref,
    part_ref, reach_ref, state_ref, total_ref,
    x_ref, wq_ref, wf_ref, wv_ref, normed_ref, q_ref, f_ref, v_ref, carry_ref, sems,
):
    pairs = ((x_hbm, x_ref), (wf_hbm, wf_ref), (wq_hbm, wq_ref), (wv_hbm, wv_ref))
    copies = [pltpu.make_async_copy(a, b, sems.at[i]) for i, (a, b) in enumerate(pairs)]
    for copy in copies:
        copy.start()
    rows, width = q_ref.shape
    blocks = rows // SPAN
    heads = width // HEAD
    gain = gain_ref[...]

    def norm_block(n, carry):
        at = pl.ds(n * SPAN, SPAN)
        normed_ref[at, :] = norm_rows(x_ref[at, :], gain)
        return carry

    copies[0].wait()
    lax.fori_loop(0, blocks, norm_block, 0)
    normed = normed_ref[...]
    copies[1].wait()
    f_ref[...] = dot(normed, wf_ref[...])
    copies[2].wait()
    q_ref[...] = dot(normed, wq_ref[...])
    copies[3].wait()
    v_ref[...] = dot(normed, wv_ref[...])
    room = room_ref[...]
    diagonal = same_head(width, width).astype(f32)
    row_at = lax.broadcasted_iota(jnp.int32, (width, SPAN), 0) % SPAN
    causal = row_at >= lax.broadcasted_iota(jnp.int32, (width, SPAN), 1)
    lower = (
        lax.broadcasted_iota(jnp.int32, (SPAN, SPAN), 0)
        >= lax.broadcasted_iota(jnp.int32, (SPAN, SPAN), 1)
    ).astype(f32)
    carry_ref[...] = jnp.zeros((width, width), f32)

    def one_block(n, log_before):
        at = pl.ds(pl.multiple_of(n * SPAN, SPAN), SPAN)
        state = carry_ref[...]
        queries = jax.nn.silu(q_ref[at, :])
        rate = room * jax.nn.sigmoid(-(f_ref[at, :] + shift_ref[n * SPAN]))
        values = v_ref[at, :].astype(bf16)
        log_decay = dot(lower, jnp.log1p(-rate), precision=lax.Precision.HIGHEST)
        middle = log_decay[SPAN // 2 : SPAN // 2 + 1]
        block_end = log_decay[SPAN - 1 :]
        from_middle = queries * jnp.exp(log_decay - middle)
        to_middle = (rate * jnp.exp(middle - log_decay)).astype(bf16)
        by_head = (jnp.concatenate([from_middle] * heads, axis=0) * diagonal).astype(bf16)
        scores = jnp.where(causal, dot(by_head, to_middle, 1, 1), 0.0).astype(bf16)
        all_pairs = dot(scores, values) * diagonal
        mixed = all_pairs[:SPAN]
        for h in range(1, heads):
            mixed = mixed + all_pairs[h * SPAN : (h + 1) * SPAN]
        decayed = queries * jnp.exp(log_decay)
        part_ref[at, :] = mixed + dot(decayed.astype(bf16), state.astype(bf16), 1, 1)
        reach_ref[at, :] = (decayed * jnp.exp(log_before)).astype(bf16)
        to_end = (rate * jnp.exp(block_end - log_decay)).astype(bf16)
        carry_ref[...] = state * jnp.exp(block_end) + dot(values, to_end, 0, 0) * diagonal
        return log_before + block_end

    log_before = lax.fori_loop(0, blocks, one_block, jnp.zeros((1, width), f32), unroll=2)
    packed = carry_ref[:HEAD]
    for h in range(1, heads):
        packed = packed + carry_ref[h * HEAD : (h + 1) * HEAD]
    state_ref[...] = packed
    total_ref[...] = jnp.exp(log_before)


def mixer_local(mix_in, shifts, gain, w_query, w_forget, w_value, room):
    rows = mix_in.shape[0]
    width = w_query.shape[1]
    vmem = pl.BlockSpec(memory_space=pltpu.VMEM)
    hbm = pl.BlockSpec(memory_space=pltpu.HBM)
    return pl.pallas_call(
        mixer_local_body,
        in_specs=[pl.BlockSpec(memory_space=pltpu.SMEM), hbm, vmem, hbm, hbm, hbm, vmem],
        out_specs=[vmem] * 4,
        out_shape=[
            jax.ShapeDtypeStruct((rows, width), f32),
            jax.ShapeDtypeStruct((rows, width), bf16),
            jax.ShapeDtypeStruct((HEAD, width), f32),
            jax.ShapeDtypeStruct((1, width), f32),
        ],
        scratch_shapes=[pltpu.VMEM(mix_in.shape, bf16)]
        + [pltpu.VMEM(w_query.shape, bf16)] * 3
        + [pltpu.VMEM(mix_in.shape, bf16)]
        + [pltpu.VMEM((rows, width), f32)] * 3
        + [pltpu.VMEM((width, width), f32), pltpu.SemaphoreType.DMA((4,))],
        compiler_params=pltpu.CompilerParams(vmem_limit_bytes=60 << 20),
        cost_estimate=pl.CostEstimate(
            flops=rows * mix_in.shape[1] * width * 6, bytes_accessed=6 << 20, transcendentals=0
        ),
        name="mixer_local",
    )(shifts, mix_in, gain, w_query, w_forget, w_value, room)


def state_scan_body(got_ref, out_ref):
    def step(i, state):
        tile = got_ref[i].astype(f32)
        out_ref[i] = state.astype(bf16)
        added = tile[0:2] + tile[2:4]
        decay = tile[4:6] + tile[6:8]
        return decay * state + added

    lax.fori_loop(0, got_ref.shape[0], step, jnp.zeros((2, 128), f32), unroll=8)


def state_scan(arrived, pieces):
    peers = arrived.shape[0]
    return pl.pallas_call(
        state_scan_body,
        grid=(1,),
        in_specs=[pl.BlockSpec((peers, 8, 128), lambda i: (0, pieces // 8, 0))],
        out_specs=pl.BlockSpec((peers, 2, 128), lambda i: (0, 0, 0)),
        out_shape=jax.ShapeDtypeStruct((peers, 2, 128), bf16),
        compiler_params=pltpu.CompilerParams(vmem_limit_bytes=8 << 20),
        name="state_scan",
    )(arrived)


def mixer_out_body(
    rank_ref, part_hbm, reach_hbm, state_ref, gain_ref, w_hbm, shared_hbm,
    own_hbm, above_hbm, top_hbm, low_hbm, below_hbm,
    part_ref, reach_ref, w_ref, shared_ref, out_ref, in_sems, out_sems,
):
    sources = ((reach_hbm, reach_ref), (part_hbm, part_ref), (w_hbm, w_ref), (shared_hbm, shared_ref))
    loads = [pltpu.make_async_copy(a, b, in_sems.at[i]) for i, (a, b) in enumerate(sources)]
    for load in loads:
        load.start()
    count, size, _ = out_ref.shape
    width = part_ref.shape[1]
    rows, tokens = part_ref.shape[0] // count, shared_ref.shape[0] // count
    heads = width // HEAD
    half = size // 2
    diagonal = same_head(width, width).astype(f32)
    state = (jnp.concatenate([state_ref[...].astype(f32)] * heads, axis=0) * diagonal).astype(bf16)
    average = diagonal * (1.0 / HEAD)
    for load in loads:
        load.wait()
    stores = []

    def store(source, target):
        stores.append(pltpu.make_async_copy(source, target, out_sems.at[len(stores)]))
        stores[-1].start()

    for i in (2, 1, 3, 0):
        rank = (rank_ref[0] + i) % count
        at = pl.ds(pl.multiple_of(rank * rows, rows), rows)
        mixed = part_ref[at, :] + dot(reach_ref[at, :], state, 1, 1)
        square = dot(mixed * mixed, average, precision=lax.Precision.HIGHEST)
        head_out = (mixed * lax.rsqrt(square + epsilon) * gain_ref[...]).astype(bf16)
        out_ref[i, :rows] = dot(head_out, w_ref[...]).astype(bf16)
        out_ref[i, rows:] = shared_ref[pl.ds(pl.multiple_of(rank * tokens, tokens), tokens), :]
        if i == 2:
            store(out_ref.at[i, pl.ds(0, half)], top_hbm)
            store(out_ref.at[i, pl.ds(half, half)], low_hbm)
        else:
            store(out_ref.at[i], {1: above_hbm, 3: below_hbm, 0: own_hbm}[i])
    for copy in stores:
        copy.wait()


def mixer_out(rank, part, reach, state, gain, w_out, shared, tp_count):
    rows, width = part.shape
    size = (rows + shared.shape[0]) // tp_count
    model = w_out.shape[1]
    sizes = [size, size, size // 2, size // 2, size]
    vmem = pl.BlockSpec(memory_space=pltpu.VMEM)
    hbm = pl.BlockSpec(memory_space=pltpu.HBM)
    return pl.pallas_call(
        mixer_out_body,
        in_specs=[pl.BlockSpec(memory_space=pltpu.SMEM), hbm, hbm, vmem, vmem, hbm, hbm],
        out_specs=[hbm] * 5,
        out_shape=[jax.ShapeDtypeStruct((n, model), bf16) for n in sizes],
        scratch_shapes=[
            pltpu.VMEM(part.shape, f32),
            pltpu.VMEM(reach.shape, bf16),
            pltpu.VMEM(w_out.shape, bf16),
            pltpu.VMEM(shared.shape, bf16),
            pltpu.VMEM((tp_count, size, model), bf16),
            pltpu.SemaphoreType.DMA((4,)),
            pltpu.SemaphoreType.DMA((5,)),
        ],
        compiler_params=pltpu.CompilerParams(vmem_limit_bytes=56 << 20),
        cost_estimate=pl.CostEstimate(
            flops=rows * width * model * 2, bytes_accessed=6 << 20, transcendentals=0
        ),
        name="mixer_out",
    )(rank, part, reach, state, gain, w_out, shared)


def narrow_out(rows_ref, tiles_ref, out_hbm, sems):
    peers, pieces, _ = tiles_ref.shape
    parts = sems.shape[0]
    part = peers // parts
    copies = []
    for i in range(parts):

        def narrow(j, carry, i=i):
            peer = i * part + j
            at = pl.multiple_of(peer * pieces, 8)
            tiles_ref[peer] = rows_ref[pl.ds(at, pieces), :].astype(bf16)
            return carry

        lax.fori_loop(0, part, narrow, 0, unroll=2)
        at = pl.ds(i * part, part)
        copies.append(pltpu.make_async_copy(tiles_ref.at[at], out_hbm.at[at], sems.at[i]))
        copies[-1].start()
    return copies


def dispatch_body(
    rank_ref, x_ref, choice_ref, gain_ref, state_ref, total_ref, out_hbm, slot_hbm,
    rows_ref, high_ref, tiles_ref, slot_ref, sems, slot_sem,
):
    quarter, model = x_ref.shape
    experts, stride, _ = tiles_ref.shape
    capacity = (stride - 8) * 128 // model
    per_row = model // 128
    hidden = norm_rows(x_ref[...], gain_ref[...])
    expert_at = lax.broadcasted_iota(jnp.int32, (quarter, experts), 1)
    chosen = [choice_ref[:, k : k + 1] == expert_at for k in range(TOP_K)]
    named = sum(one.astype(f32) for one in chosen)
    earlier = lax.broadcasted_iota(jnp.int32, (quarter, quarter), 0) > lax.broadcasted_iota(
        jnp.int32, (quarter, quarter), 1
    )
    ranks = dot(earlier.astype(bf16), named.astype(bf16))
    for k in range(TOP_K):
        place = jnp.sum(jnp.where(chosen[k], ranks, 0.0), axis=-1, keepdims=True)
        slot_ref[:, k : k + 1] = choice_ref[:, k : k + 1] * capacity + place.astype(jnp.int32)
    for c in range(capacity):
        holds = jnp.where(ranks == c, named, 0.0).astype(bf16)
        rows = dot(holds, hidden, 0, 0)
        for k in range(per_row):
            rows_ref[pl.ds(c * per_row + k, experts, stride=stride), :] = rows[
                :, k * 128 : (k + 1) * 128
            ]
    base = stride - 8
    total = jnp.broadcast_to(total_ref[...], state_ref.shape)
    high_ref[0] = state_ref[...].astype(bf16)
    high_ref[1] = total.astype(bf16)
    state_high = high_ref[0].astype(f32)
    total_high = high_ref[1].astype(f32)
    sent = (state_high, state_ref[...] - state_high, total_high, total - total_high)
    for i, part in enumerate(sent):
        for j in range(2):
            rows_ref[pl.ds(base + 2 * i + j, experts, stride=stride), :] = part[
                :, j * 128 : (j + 1) * 128
            ]

    slot_copy = pltpu.make_async_copy(slot_ref, slot_hbm, slot_sem)
    slot_copy.start()
    for copy in narrow_out(rows_ref, tiles_ref, out_hbm, sems) + [slot_copy]:
        copy.wait()


def dispatch(rank, moe_in, choice, gain, state, total, quarter, experts, pieces):
    model = moe_in.shape[1]
    mine = lambda i, rank: (rank[0], 0)
    whole = lambda i, rank: (0, 0)
    return pl.pallas_call(
        dispatch_body,
        grid_spec=pltpu.PrefetchScalarGridSpec(
            num_scalar_prefetch=1,
            grid=(1,),
            in_specs=[
                pl.BlockSpec((quarter, model), mine),
                pl.BlockSpec((quarter, TOP_K), mine),
                pl.BlockSpec((1, model), whole),
                pl.BlockSpec(state.shape, whole),
                pl.BlockSpec(total.shape, whole),
            ],
            out_specs=[pl.BlockSpec(memory_space=pltpu.HBM)] * 2,
            scratch_shapes=[
                pltpu.VMEM((experts * (pieces + 8), 128), f32),
                pltpu.VMEM((2, *state.shape), bf16),
                pltpu.VMEM((experts, pieces + 8, 128), bf16),
                pltpu.VMEM((quarter, TOP_K), jnp.int32),
                pltpu.SemaphoreType.DMA((4,)),
                pltpu.SemaphoreType.DMA,
            ],
        ),
        out_shape=[
            jax.ShapeDtypeStruct((experts, pieces + 8, 128), bf16),
            jax.ShapeDtypeStruct((quarter, TOP_K), jnp.int32),
        ],
        compiler_params=pltpu.CompilerParams(vmem_limit_bytes=60 << 20),
        name="dispatch",
    )(rank, moe_in, choice, gain, state, total)


def widen_rows(tiles_ref, rows_ref, start, count):
    pieces = rows_ref.shape[0] // tiles_ref.shape[0]

    def widen(i, carry):
        at = pl.multiple_of((start + i) * pieces, 8)
        rows_ref[pl.ds(at, pieces), :] = tiles_ref[start + i, :pieces].astype(f32)
        return carry

    lax.fori_loop(0, count, widen, 0, unroll=2)


def gather_rows(rows_ref, x_ref, peers):
    slots, model = x_ref.shape
    capacity = slots // peers
    per_row = model // 128
    for c in range(capacity):
        for k in range(per_row):
            x_ref[c * peers : (c + 1) * peers, k * 128 : (k + 1) * 128] = rows_ref[
                pl.ds(c * per_row + k, peers, stride=capacity * per_row), :
            ].astype(bf16)


def hidden_units_body(got_ref, *refs):
    groups = (len(refs) - 3) // 2
    gates, ups = refs[:groups], refs[groups : 2 * groups]
    out_ref, rows_ref, x_ref = refs[2 * groups :]
    peers = got_ref.shape[0]
    width = gates[0].shape[1]
    widen_rows(got_ref, rows_ref, 0, peers)
    gather_rows(rows_ref, x_ref, peers)
    x = x_ref[...]
    for i in range(groups):
        act = jax.nn.silu(dot(x, gates[i][...])) * dot(x, ups[i][...])
        out_ref[:, i * width : (i + 1) * width] = act.astype(bf16)


def hidden_units(arrived, gates, ups, pieces):
    peers = arrived.shape[0]
    model, width = gates[0].shape
    slots = peers * pieces * 128 // model
    groups = len(gates)
    whole = lambda i: (0, 0)
    return pl.pallas_call(
        hidden_units_body,
        grid=(1,),
        in_specs=[pl.BlockSpec((peers, pieces, 128), lambda i: (0, 0, 0))]
        + [pl.BlockSpec((model, width), whole)] * (2 * groups),
        out_specs=pl.BlockSpec((slots, groups * width), whole),
        out_shape=jax.ShapeDtypeStruct((slots, groups * width), bf16),
        scratch_shapes=[pltpu.VMEM((peers * pieces, 128), f32), pltpu.VMEM((slots, model), bf16)],
        compiler_params=pltpu.CompilerParams(vmem_limit_bytes=56 << 20),
        cost_estimate=pl.CostEstimate(
            flops=slots * model * width * 4 * groups,
            bytes_accessed=10 << 20,
            transcendentals=0,
        ),
        name="hidden_units",
    )(arrived, *gates, *ups)


def results_body(act_ref, *refs):
    halves = refs[:-6]
    out_hbm, weight_ref, rows_ref, tiles_ref, sems, out_sems = refs[-6:]
    peers, pieces, _ = tiles_ref.shape
    slots = act_ref.shape[0]
    half, model = halves[0].shape
    capacity = slots // peers
    per_row = model // 128
    parts = sems.shape[0]
    part = model // parts
    loads = [
        [
            pltpu.make_async_copy(
                ref.at[:, pl.ds(i * part, part)],
                weight_ref.at[i, pl.ds(j * half, half)],
                sems.at[i, j],
            )
            for j, ref in enumerate(halves)
        ]
        for i in range(parts)
    ]
    for group in loads:
        for load in group:
            load.start()
    for i in range(parts):
        for load in loads[i]:
            load.wait()
        whole = dot(act_ref[...], weight_ref[i])
        for c in range(capacity):
            for j in range(part // 128):
                k = (i * part) // 128 + j
                rows_ref[pl.ds(c * per_row + k, peers, stride=pieces), :] = whole[
                    c * peers : (c + 1) * peers, j * 128 : (j + 1) * 128
                ]
    for copy in narrow_out(rows_ref, tiles_ref, out_hbm, out_sems):
        copy.wait()


def results(acts, halves, peers):
    slots, width = acts.shape
    _, model = halves[0].shape
    pieces = slots // peers * model // 128
    hbm = pl.BlockSpec(memory_space=pltpu.HBM)
    parts = 4
    return pl.pallas_call(
        results_body,
        in_specs=[pl.BlockSpec(memory_space=pltpu.VMEM)] + [hbm] * len(halves),
        out_specs=hbm,
        out_shape=jax.ShapeDtypeStruct((peers, pieces, 128), bf16),
        scratch_shapes=[
            pltpu.VMEM((parts, width, model // parts), bf16),
            pltpu.VMEM((peers * pieces, 128), f32),
            pltpu.VMEM((peers, pieces, 128), bf16),
            pltpu.SemaphoreType.DMA((parts, len(halves))),
            pltpu.SemaphoreType.DMA((4,)),
        ],
        compiler_params=pltpu.CompilerParams(vmem_limit_bytes=20 << 20),
        cost_estimate=pl.CostEstimate(
            flops=slots * model * width * 2, bytes_accessed=6 << 20, transcendentals=0
        ),
        name="results",
    )(acts, *halves)


def combine_body(got_ref, slot_ref, logit_ref, rest_ref, out_ref, rows_ref, x_ref, split_ref):
    peers = got_ref.shape[0]
    slots = x_ref.shape[0]
    capacity = slots // peers
    widen_rows(got_ref, rows_ref, 0, peers)
    gather_rows(rows_ref, x_ref, peers)
    chance = jax.nn.sigmoid(logit_ref[...])
    weights = chance / jnp.sum(chance, axis=-1, keepdims=True) * route_scale
    tokens = weights.shape[0]
    first = lax.broadcasted_iota(jnp.int32, (tokens, peers), 1) * capacity
    picks = []
    for c in range(capacity):
        picks.append(
            sum(
                jnp.where(slot_ref[:, k : k + 1] == first + c, weights[:, k : k + 1], 0.0)
                for k in range(TOP_K)
            )
        )
    pick = jnp.concatenate(picks, axis=1)
    split_ref[0] = pick.astype(bf16)
    split_ref[1] = (pick - split_ref[0].astype(f32)).astype(bf16)
    x = x_ref[...]
    routed = dot(split_ref[0], x) + dot(split_ref[1], x)
    out_ref[...] = (routed + rest_ref[...]).astype(bf16)


def combine(returned, slot_ids, route_logit, rest):
    peers, pieces, _ = returned.shape
    tokens, model = rest.shape
    slots = peers * pieces * 128 // model
    return pl.pallas_call(
        combine_body,
        out_shape=jax.ShapeDtypeStruct((tokens, model), bf16),
        scratch_shapes=[
            pltpu.VMEM((peers * pieces, 128), f32),
            pltpu.VMEM((slots, model), bf16),
            pltpu.VMEM((2, tokens, slots), bf16),
        ],
        compiler_params=pltpu.CompilerParams(vmem_limit_bytes=16 << 20),
        name="combine",
    )(returned, slot_ids, route_logit, rest)


def shift_up(x):
    return lax.ppermute(x, "tp", UP)


def shift_down(x):
    return lax.ppermute(x, "tp", DOWN)


def after(x, *others):
    return lax.optimization_barrier((x, *others))[0]


def local(
    mix_in,
    forget_shift,
    mix_gain,
    w_query,
    w_forget,
    w_value,
    forget_room,
    head_gain,
    w_out,
    moe_in,
    moe_gain,
    expert_choice,
    route_logit,
    w_exp_gate,
    w_exp_up,
    w_exp_down,
    w_sh_gate,
    w_sh_up,
    w_sh_down,
):
    tp_count = 4
    tp_rank = lax.axis_index("tp")
    row_count, model = moe_in.shape
    quarter = row_count // tp_count
    experts = lax.axis_size(EP) * w_exp_gate.shape[0]
    mean_load = quarter * TOP_K // experts
    capacity = mean_load + mean_load // 2
    pieces = capacity * model // 128

    gate_own, up_own, down_own = w_exp_gate[0], w_exp_up[0], w_exp_down[0]
    gate_below = shift_up(gate_own)
    up_above = shift_down(up_own)
    up_below = shift_up(up_own)
    gate_above = shift_down(gate_own)
    gate_far = shift_up(gate_below)
    up_far = shift_down(up_above)
    half_units = down_own.shape[0] // 2
    top, low = down_own[:half_units], down_own[half_units:]
    top_below = shift_up(top)
    low_above = shift_down(low)
    low_below = shift_up(low)
    top_above = shift_down(top)

    part, reach, added, total = mixer_local(
        mix_in, forget_shift, mix_gain[None], w_query, w_forget, w_value, forget_room[None]
    )
    outgoing, slot_ids = dispatch(
        tp_rank.reshape(1), moe_in, expert_choice, moe_gain[None], added, total,
        quarter, experts, pieces,
    )
    arrived = lax.all_to_all(outgoing, EP, split_axis=0, concat_axis=0, tiled=True)
    hidden = norm_rows(moe_in, moe_gain)
    shared_gate = dot(hidden, w_sh_gate)
    shared_up = dot(hidden, w_sh_up)
    shared_act = (jax.nn.silu(shared_gate) * shared_up).astype(bf16)
    shared_part = dot(shared_act, w_sh_down).astype(bf16)
    arrived = after(arrived, shared_part)
    state_next = state_scan(arrived, pieces)
    top_far = shift_up(after(top_below, state_next))
    low_far = shift_down(after(low_above, state_next))
    state_start = lax.all_to_all(state_next, EP, split_axis=0, concat_axis=0, tiled=True)
    state_start = state_start.reshape(HEAD, -1)
    own, to_above, across_top, across_low, to_below = mixer_out(
        tp_rank.reshape(1), part, reach, state_start, head_gain[None], w_out, shared_part, tp_count
    )

    acts = hidden_units(
        arrived,
        [gate_own, gate_below, gate_above, gate_far],
        [up_own, up_below, up_above, up_far],
        pieces,
    )
    ready = results(
        acts,
        [top, low, top_below, low_below, top_above, low_above, top_far, low_far],
        experts,
    )
    returned = lax.all_to_all(ready, EP, split_axis=0, concat_axis=0, tiled=True)

    middle = across_top.shape[0]
    via_below = shift_up(across_top)
    via_above = shift_down(across_low)
    to_above = jnp.concatenate([to_above[:middle] + via_below, to_above[middle:]], axis=0)
    to_below = jnp.concatenate([to_below[:middle], to_below[middle:] + via_above], axis=0)
    from_below = shift_up(to_above)
    from_above = shift_down(to_below)
    total_rows = own.astype(f32) + from_below.astype(f32) + from_above.astype(f32)
    mixer_rows = mix_in.shape[0] // tp_count
    return (
        total_rows[:mixer_rows].astype(bf16),
        combine(returned, slot_ids, route_logit, total_rows[mixer_rows:]),
    )


def solution(mesh):
    finer = Mesh(mesh.devices.reshape(8, 4, 2, mesh.shape["tp"]), ("ep_0", "ep_1", "ep_2", "tp"))
    in_specs = (
        P(EP, None),
        P(EP),
        P(),
        P(None, "tp"),
        P(None, "tp"),
        P(None, "tp"),
        P("tp"),
        P("tp"),
        P("tp", None),
        P(EP, None),
        P(),
        P(EP, None),
        P(EP_TP, None),
        P(EP, None, "tp"),
        P(EP, None, "tp"),
        P(EP, "tp", None),
        P(None, "tp"),
        P(None, "tp"),
        P("tp", None),
    )
    out_specs = (P(EP_TP, None), P(EP_TP, None))

    return jax.shard_map(local, mesh=finer, in_specs=in_specs, out_specs=out_specs, check_vma=False)
```

```python
import jax
import jax.numpy as jnp
from jax import lax
from jax.experimental import pallas as pl
from jax.experimental.pallas import tpu as pltpu
from jax.sharding import Mesh
from jax.sharding import PartitionSpec as P

HEAD = 64
SPAN = 64
TOP_K = 4
EP = ("ep_0", "ep_1", "ep_2")
EP_TP = ("ep_0", "ep_1", "ep_2", "tp")
UP = [(i, (i + 1) % 4) for i in range(4)]
DOWN = [(i, (i - 1) % 4) for i in range(4)]

epsilon = 1e-06
route_scale = 2.5
f32 = jnp.float32
bf16 = jnp.bfloat16


def dot(a, b, ca=1, cb=0, **kw):
    return lax.dot_general(a, b, (((ca,), (cb,)), ((), ())), preferred_element_type=f32, **kw)


def norm_rows(row_data, gain_vec):
    widened = row_data.astype(f32)
    scaled = widened * lax.rsqrt(jnp.mean(widened * widened, axis=-1, keepdims=True) + epsilon)
    return (scaled * gain_vec).astype(bf16)


def same_head(rows, cols):
    row_head = lax.broadcasted_iota(jnp.int32, (rows, cols), 0) // HEAD
    col_head = lax.broadcasted_iota(jnp.int32, (rows, cols), 1) // HEAD
    return row_head == col_head


def mixer_local_body(
    shift_ref, x_ref, gain_ref, wq_ref, wf_ref, wv_ref, room_ref,
    part_ref, reach_ref, state_ref, total_ref,
    normed_ref, q_ref, f_ref, v_ref, carry_ref,
):
    rows, width = q_ref.shape
    blocks = rows // SPAN
    heads = width // HEAD
    gain = gain_ref[...]

    def norm_block(n, carry):
        at = pl.ds(n * SPAN, SPAN)
        normed_ref[at, :] = norm_rows(x_ref[at, :], gain)
        return carry

    lax.fori_loop(0, blocks, norm_block, 0)
    normed = normed_ref[...]
    f_ref[...] = dot(normed, wf_ref[...])
    q_ref[...] = dot(normed, wq_ref[...])
    v_ref[...] = dot(normed, wv_ref[...])
    room = room_ref[...]
    diagonal = same_head(width, width).astype(f32)
    row_at = lax.broadcasted_iota(jnp.int32, (width, SPAN), 0) % SPAN
    causal = row_at >= lax.broadcasted_iota(jnp.int32, (width, SPAN), 1)
    lower = (
        lax.broadcasted_iota(jnp.int32, (SPAN, SPAN), 0)
        >= lax.broadcasted_iota(jnp.int32, (SPAN, SPAN), 1)
    ).astype(f32)
    carry_ref[...] = jnp.zeros((width, width), f32)

    def one_block(n, log_before):
        at = pl.ds(pl.multiple_of(n * SPAN, SPAN), SPAN)
        state = carry_ref[...]
        queries = jax.nn.silu(q_ref[at, :])
        rate = room * jax.nn.sigmoid(-(f_ref[at, :] + shift_ref[n * SPAN]))
        values = v_ref[at, :].astype(bf16)
        log_decay = dot(lower, jnp.log1p(-rate), precision=lax.Precision.HIGHEST)
        middle = log_decay[SPAN // 2 : SPAN // 2 + 1]
        block_end = log_decay[SPAN - 1 :]
        from_middle = queries * jnp.exp(log_decay - middle)
        to_middle = (rate * jnp.exp(middle - log_decay)).astype(bf16)
        by_head = (jnp.concatenate([from_middle] * heads, axis=0) * diagonal).astype(bf16)
        scores = jnp.where(causal, dot(by_head, to_middle, 1, 1), 0.0).astype(bf16)
        all_pairs = dot(scores, values) * diagonal
        mixed = all_pairs[:SPAN]
        for h in range(1, heads):
            mixed = mixed + all_pairs[h * SPAN : (h + 1) * SPAN]
        decayed = queries * jnp.exp(log_decay)
        part_ref[at, :] = mixed + dot(decayed.astype(bf16), state.astype(bf16), 1, 1)
        reach_ref[at, :] = (decayed * jnp.exp(log_before)).astype(bf16)
        to_end = (rate * jnp.exp(block_end - log_decay)).astype(bf16)
        carry_ref[...] = state * jnp.exp(block_end) + dot(values, to_end, 0, 0) * diagonal
        return log_before + block_end

    log_before = lax.fori_loop(0, blocks, one_block, jnp.zeros((1, width), f32), unroll=2)
    packed = carry_ref[:HEAD]
    for h in range(1, heads):
        packed = packed + carry_ref[h * HEAD : (h + 1) * HEAD]
    state_ref[...] = packed
    total_ref[...] = jnp.exp(log_before)


def mixer_local(mix_in, shifts, gain, w_query, w_forget, w_value, room):
    rows = mix_in.shape[0]
    width = w_query.shape[1]
    vmem = pl.BlockSpec(memory_space=pltpu.VMEM)
    hbm = pl.BlockSpec(memory_space=pltpu.HBM)
    return pl.pallas_call(
        mixer_local_body,
        grid=(1,),
        in_specs=[pl.BlockSpec(memory_space=pltpu.SMEM)]
        + [
            pl.BlockSpec(x.shape, lambda i: (0, 0))
            for x in (mix_in, gain, w_query, w_forget, w_value, room)
        ],
        out_specs=[vmem] * 4,
        out_shape=[
            jax.ShapeDtypeStruct((rows, width), f32),
            jax.ShapeDtypeStruct((rows, width), bf16),
            jax.ShapeDtypeStruct((HEAD, width), f32),
            jax.ShapeDtypeStruct((1, width), f32),
        ],
        scratch_shapes=[pltpu.VMEM(mix_in.shape, bf16)]
        + [pltpu.VMEM((rows, width), f32)] * 3
        + [pltpu.VMEM((width, width), f32)],
        compiler_params=pltpu.CompilerParams(vmem_limit_bytes=60 << 20),
        cost_estimate=pl.CostEstimate(
            flops=rows * mix_in.shape[1] * width * 6, bytes_accessed=6 << 20, transcendentals=0
        ),
        name="mixer_local",
    )(shifts, mix_in, gain, w_query, w_forget, w_value, room)


def state_scan_body(got_ref, out_ref):
    def step(i, state):
        tile = got_ref[i].astype(f32)
        out_ref[i] = state.astype(bf16)
        added = tile[0:2] + tile[2:4]
        decay = tile[4:6] + tile[6:8]
        return decay * state + added

    lax.fori_loop(0, got_ref.shape[0], step, jnp.zeros((2, 128), f32), unroll=8)


def state_scan(arrived, pieces):
    peers = arrived.shape[0]
    return pl.pallas_call(
        state_scan_body,
        grid=(1,),
        in_specs=[pl.BlockSpec((peers, 8, 128), lambda i: (0, pieces // 8, 0))],
        out_specs=pl.BlockSpec((peers, 2, 128), lambda i: (0, 0, 0)),
        out_shape=jax.ShapeDtypeStruct((peers, 2, 128), bf16),
        compiler_params=pltpu.CompilerParams(vmem_limit_bytes=8 << 20),
        name="state_scan",
    )(arrived)


def mixer_out_body(
    rank_ref, part_hbm, reach_hbm, state_ref, gain_ref, w_hbm, shared_hbm,
    own_hbm, above_hbm, top_hbm, low_hbm, below_hbm,
    part_ref, reach_ref, w_ref, shared_ref, out_ref, in_sems, out_sems,
):
    sources = ((reach_hbm, reach_ref), (part_hbm, part_ref), (w_hbm, w_ref), (shared_hbm, shared_ref))
    loads = [pltpu.make_async_copy(a, b, in_sems.at[i]) for i, (a, b) in enumerate(sources)]
    for load in loads:
        load.start()
    count, size, _ = out_ref.shape
    width = part_ref.shape[1]
    rows, tokens = part_ref.shape[0] // count, shared_ref.shape[0] // count
    heads = width // HEAD
    half = size // 2
    diagonal = same_head(width, width).astype(f32)
    state = (jnp.concatenate([state_ref[...].astype(f32)] * heads, axis=0) * diagonal).astype(bf16)
    average = diagonal * (1.0 / HEAD)
    for load in loads:
        load.wait()
    stores = []

    def store(source, target):
        stores.append(pltpu.make_async_copy(source, target, out_sems.at[len(stores)]))
        stores[-1].start()

    for i in (2, 1, 3, 0):
        rank = (rank_ref[0] + i) % count
        at = pl.ds(pl.multiple_of(rank * rows, rows), rows)
        mixed = part_ref[at, :] + dot(reach_ref[at, :], state, 1, 1)
        square = dot(mixed * mixed, average, precision=lax.Precision.HIGHEST)
        head_out = (mixed * lax.rsqrt(square + epsilon) * gain_ref[...]).astype(bf16)
        out_ref[i, :rows] = dot(head_out, w_ref[...]).astype(bf16)
        out_ref[i, rows:] = shared_ref[pl.ds(pl.multiple_of(rank * tokens, tokens), tokens), :]
        if i == 2:
            store(out_ref.at[i, pl.ds(0, half)], top_hbm)
            store(out_ref.at[i, pl.ds(half, half)], low_hbm)
        else:
            store(out_ref.at[i], {1: above_hbm, 3: below_hbm, 0: own_hbm}[i])
    for copy in stores:
        copy.wait()


def mixer_out(rank, part, reach, state, gain, w_out, shared, tp_count):
    rows, width = part.shape
    size = (rows + shared.shape[0]) // tp_count
    model = w_out.shape[1]
    sizes = [size, size, size // 2, size // 2, size]
    vmem = pl.BlockSpec(memory_space=pltpu.VMEM)
    hbm = pl.BlockSpec(memory_space=pltpu.HBM)
    return pl.pallas_call(
        mixer_out_body,
        in_specs=[pl.BlockSpec(memory_space=pltpu.SMEM), hbm, hbm, vmem, vmem, hbm, hbm],
        out_specs=[hbm] * 5,
        out_shape=[jax.ShapeDtypeStruct((n, model), bf16) for n in sizes],
        scratch_shapes=[
            pltpu.VMEM(part.shape, f32),
            pltpu.VMEM(reach.shape, bf16),
            pltpu.VMEM(w_out.shape, bf16),
            pltpu.VMEM(shared.shape, bf16),
            pltpu.VMEM((tp_count, size, model), bf16),
            pltpu.SemaphoreType.DMA((4,)),
            pltpu.SemaphoreType.DMA((5,)),
        ],
        compiler_params=pltpu.CompilerParams(vmem_limit_bytes=56 << 20),
        cost_estimate=pl.CostEstimate(
            flops=rows * width * model * 2, bytes_accessed=6 << 20, transcendentals=0
        ),
        name="mixer_out",
    )(rank, part, reach, state, gain, w_out, shared)


def narrow_out(rows_ref, tiles_ref, out_hbm, sems):
    peers, pieces, _ = tiles_ref.shape
    parts = sems.shape[0]
    part = peers // parts
    copies = []
    for i in range(parts):

        def narrow(j, carry, i=i):
            peer = i * part + j
            at = pl.multiple_of(peer * pieces, 8)
            tiles_ref[peer] = rows_ref[pl.ds(at, pieces), :].astype(bf16)
            return carry

        lax.fori_loop(0, part, narrow, 0, unroll=2)
        at = pl.ds(i * part, part)
        copies.append(pltpu.make_async_copy(tiles_ref.at[at], out_hbm.at[at], sems.at[i]))
        copies[-1].start()
    return copies


def dispatch_body(
    rank_ref, x_ref, choice_ref, gain_ref, state_ref, total_ref, out_hbm, slot_hbm,
    rows_ref, high_ref, tiles_ref, slot_ref, sems, slot_sem,
):
    quarter, model = x_ref.shape
    experts, stride, _ = tiles_ref.shape
    capacity = (stride - 8) * 128 // model
    per_row = model // 128
    hidden = norm_rows(x_ref[...], gain_ref[...])
    expert_at = lax.broadcasted_iota(jnp.int32, (quarter, experts), 1)
    chosen = [choice_ref[:, k : k + 1] == expert_at for k in range(TOP_K)]
    named = sum(one.astype(f32) for one in chosen)
    earlier = lax.broadcasted_iota(jnp.int32, (quarter, quarter), 0) > lax.broadcasted_iota(
        jnp.int32, (quarter, quarter), 1
    )
    ranks = dot(earlier.astype(bf16), named.astype(bf16))
    for k in range(TOP_K):
        place = jnp.sum(jnp.where(chosen[k], ranks, 0.0), axis=-1, keepdims=True)
        slot_ref[:, k : k + 1] = choice_ref[:, k : k + 1] * capacity + place.astype(jnp.int32)
    for c in range(capacity):
        holds = jnp.where(ranks == c, named, 0.0).astype(bf16)
        rows = dot(holds, hidden, 0, 0)
        for k in range(per_row):
            rows_ref[pl.ds(c * per_row + k, experts, stride=stride), :] = rows[
                :, k * 128 : (k + 1) * 128
            ]
    base = stride - 8
    total = jnp.broadcast_to(total_ref[...], state_ref.shape)
    high_ref[0] = state_ref[...].astype(bf16)
    high_ref[1] = total.astype(bf16)
    state_high = high_ref[0].astype(f32)
    total_high = high_ref[1].astype(f32)
    sent = (state_high, state_ref[...] - state_high, total_high, total - total_high)
    for i, part in enumerate(sent):
        for j in range(2):
            rows_ref[pl.ds(base + 2 * i + j, experts, stride=stride), :] = part[
                :, j * 128 : (j + 1) * 128
            ]

    slot_copy = pltpu.make_async_copy(slot_ref, slot_hbm, slot_sem)
    slot_copy.start()
    for copy in narrow_out(rows_ref, tiles_ref, out_hbm, sems) + [slot_copy]:
        copy.wait()


def dispatch(rank, moe_in, choice, gain, state, total, quarter, experts, pieces):
    model = moe_in.shape[1]
    mine = lambda i, rank: (rank[0], 0)
    whole = lambda i, rank: (0, 0)
    return pl.pallas_call(
        dispatch_body,
        grid_spec=pltpu.PrefetchScalarGridSpec(
            num_scalar_prefetch=1,
            grid=(1,),
            in_specs=[
                pl.BlockSpec((quarter, model), mine),
                pl.BlockSpec((quarter, TOP_K), mine),
                pl.BlockSpec((1, model), whole),
                pl.BlockSpec(state.shape, whole),
                pl.BlockSpec(total.shape, whole),
            ],
            out_specs=[pl.BlockSpec(memory_space=pltpu.HBM)] * 2,
            scratch_shapes=[
                pltpu.VMEM((experts * (pieces + 8), 128), f32),
                pltpu.VMEM((2, *state.shape), bf16),
                pltpu.VMEM((experts, pieces + 8, 128), bf16),
                pltpu.VMEM((quarter, TOP_K), jnp.int32),
                pltpu.SemaphoreType.DMA((4,)),
                pltpu.SemaphoreType.DMA,
            ],
        ),
        out_shape=[
            jax.ShapeDtypeStruct((experts, pieces + 8, 128), bf16),
            jax.ShapeDtypeStruct((quarter, TOP_K), jnp.int32),
        ],
        compiler_params=pltpu.CompilerParams(vmem_limit_bytes=60 << 20),
        name="dispatch",
    )(rank, moe_in, choice, gain, state, total)


def widen_rows(tiles_ref, rows_ref, start, count):
    pieces = rows_ref.shape[0] // tiles_ref.shape[0]

    def widen(i, carry):
        at = pl.multiple_of((start + i) * pieces, 8)
        rows_ref[pl.ds(at, pieces), :] = tiles_ref[start + i, :pieces].astype(f32)
        return carry

    lax.fori_loop(0, count, widen, 0, unroll=2)


def gather_rows(rows_ref, x_ref, peers):
    slots, model = x_ref.shape
    capacity = slots // peers
    per_row = model // 128
    for c in range(capacity):
        for k in range(per_row):
            x_ref[c * peers : (c + 1) * peers, k * 128 : (k + 1) * 128] = rows_ref[
                pl.ds(c * per_row + k, peers, stride=capacity * per_row), :
            ].astype(bf16)


def hidden_units_body(got_ref, *refs):
    groups = (len(refs) - 3) // 2
    gates, ups = refs[:groups], refs[groups : 2 * groups]
    out_ref, rows_ref, x_ref = refs[2 * groups :]
    peers = got_ref.shape[0]
    width = gates[0].shape[1]
    widen_rows(got_ref, rows_ref, 0, peers)
    gather_rows(rows_ref, x_ref, peers)
    x = x_ref[...]
    for i in range(groups):
        act = jax.nn.silu(dot(x, gates[i][...])) * dot(x, ups[i][...])
        out_ref[:, i * width : (i + 1) * width] = act.astype(bf16)


def hidden_units(arrived, gates, ups, pieces):
    peers = arrived.shape[0]
    model, width = gates[0].shape
    slots = peers * pieces * 128 // model
    groups = len(gates)
    whole = lambda i: (0, 0)
    return pl.pallas_call(
        hidden_units_body,
        grid=(1,),
        in_specs=[pl.BlockSpec((peers, pieces, 128), lambda i: (0, 0, 0))]
        + [pl.BlockSpec((model, width), whole)] * (2 * groups),
        out_specs=pl.BlockSpec((slots, groups * width), whole),
        out_shape=jax.ShapeDtypeStruct((slots, groups * width), bf16),
        scratch_shapes=[pltpu.VMEM((peers * pieces, 128), f32), pltpu.VMEM((slots, model), bf16)],
        compiler_params=pltpu.CompilerParams(vmem_limit_bytes=56 << 20),
        cost_estimate=pl.CostEstimate(
            flops=slots * model * width * 4 * groups,
            bytes_accessed=10 << 20,
            transcendentals=0,
        ),
        name="hidden_units",
    )(arrived, *gates, *ups)


def results_body(act_ref, *refs):
    halves = refs[:-4]
    out_hbm, rows_ref, tiles_ref, sems = refs[-4:]
    peers, pieces, _ = tiles_ref.shape
    slots = act_ref.shape[0]
    model = halves[0].shape[1]
    capacity = slots // peers
    per_row = model // 128
    part = 256
    act = act_ref[...]
    for col in range(0, model, part):
        weight = jnp.concatenate([ref[:, col : col + part] for ref in halves], axis=0)
        whole = dot(act, weight)
        for c in range(capacity):
            for j in range(part // 128):
                k = col // 128 + j
                rows_ref[pl.ds(c * per_row + k, peers, stride=pieces), :] = whole[
                    c * peers : (c + 1) * peers, j * 128 : (j + 1) * 128
                ]
    for copy in narrow_out(rows_ref, tiles_ref, out_hbm, sems):
        copy.wait()


def results(acts, weights, peers):
    slots, width = acts.shape
    model = weights[0].shape[1]
    pieces = slots // peers * model // 128
    whole = lambda i: (0, 0)
    return pl.pallas_call(
        results_body,
        grid=(1,),
        in_specs=[pl.BlockSpec((slots, width), whole)]
        + [pl.BlockSpec(w.shape, whole) for w in weights],
        out_specs=pl.BlockSpec(memory_space=pltpu.HBM),
        out_shape=jax.ShapeDtypeStruct((peers, pieces, 128), bf16),
        scratch_shapes=[
            pltpu.VMEM((peers * pieces, 128), f32),
            pltpu.VMEM((peers, pieces, 128), bf16),
            pltpu.SemaphoreType.DMA((4,)),
        ],
        compiler_params=pltpu.CompilerParams(vmem_limit_bytes=60 << 20),
        cost_estimate=pl.CostEstimate(
            flops=slots * model * width * 2, bytes_accessed=6 << 20, transcendentals=0
        ),
        name="results",
    )(acts, *weights)


def combine_body(got_ref, slot_ref, logit_ref, rest_ref, out_ref, rows_ref, split_ref):
    peers = got_ref.shape[0]
    tokens, model = out_ref.shape
    slots = split_ref.shape[2]
    capacity = slots // peers
    per_row = model // 128
    widen_rows(got_ref, rows_ref, 0, peers)
    chance = jax.nn.sigmoid(logit_ref[...])
    weights = chance / jnp.sum(chance, axis=-1, keepdims=True) * route_scale
    first = lax.broadcasted_iota(jnp.int32, (tokens, peers), 1) * capacity
    picks = []
    for c in range(capacity):
        picks.append(
            sum(
                jnp.where(slot_ref[:, k : k + 1] == first + c, weights[:, k : k + 1], 0.0)
                for k in range(TOP_K)
            )
        )
    pick = jnp.concatenate(picks, axis=1)
    split_ref[0] = pick.astype(bf16)
    split_ref[1] = (pick - split_ref[0].astype(f32)).astype(bf16)
    both = jnp.concatenate([split_ref[0], split_ref[1]], axis=0)
    for k in range(0, per_row, 2):
        x = jnp.concatenate(
            [
                jnp.concatenate(
                    [
                        rows_ref[pl.ds(c * per_row + k + j, peers, stride=capacity * per_row), :]
                        for j in range(2)
                    ],
                    axis=1,
                )
                for c in range(capacity)
            ],
            axis=0,
        ).astype(bf16)
        sums = dot(both, x)
        cols = slice(k * 128, (k + 2) * 128)
        out_ref[:, cols] = (sums[:tokens] + sums[tokens:] + rest_ref[:, cols]).astype(bf16)


def combine(returned, slot_ids, route_logit, rest):
    peers, pieces, _ = returned.shape
    tokens, model = rest.shape
    slots = peers * pieces * 128 // model
    return pl.pallas_call(
        combine_body,
        out_shape=jax.ShapeDtypeStruct((tokens, model), bf16),
        scratch_shapes=[
            pltpu.VMEM((peers * pieces, 128), f32),
            pltpu.VMEM((2, tokens, slots), bf16),
        ],
        compiler_params=pltpu.CompilerParams(vmem_limit_bytes=16 << 20),
        name="combine",
    )(returned, slot_ids, route_logit, rest)


def shift_up(x):
    return lax.ppermute(x, "tp", UP)


def shift_down(x):
    return lax.ppermute(x, "tp", DOWN)


def after(x, *others):
    return lax.optimization_barrier((x, *others))[0]


def local(
    mix_in,
    forget_shift,
    mix_gain,
    w_query,
    w_forget,
    w_value,
    forget_room,
    head_gain,
    w_out,
    moe_in,
    moe_gain,
    expert_choice,
    route_logit,
    w_exp_gate,
    w_exp_up,
    w_exp_down,
    w_sh_gate,
    w_sh_up,
    w_sh_down,
):
    tp_count = 4
    tp_rank = lax.axis_index("tp")
    row_count, model = moe_in.shape
    quarter = row_count // tp_count
    experts = lax.axis_size(EP) * w_exp_gate.shape[0]
    mean_load = quarter * TOP_K // experts
    capacity = mean_load + mean_load // 2
    pieces = capacity * model // 128

    gate_own, up_own, down_own = w_exp_gate[0], w_exp_up[0], w_exp_down[0]
    gate_below = shift_up(gate_own)
    up_above = shift_down(up_own)
    up_below = shift_up(up_own)
    gate_above = shift_down(gate_own)
    gate_far = shift_up(gate_below)
    up_far = shift_down(up_above)
    half_units = down_own.shape[0] // 2
    top, low = down_own[:half_units], down_own[half_units:]
    top_below = shift_up(top)
    low_above = shift_down(low)
    low_below = shift_up(low)
    top_above = shift_down(top)

    part, reach, added, total = mixer_local(
        mix_in, forget_shift, mix_gain[None], w_query, w_forget, w_value, forget_room[None]
    )
    outgoing, slot_ids = dispatch(
        tp_rank.reshape(1), moe_in, expert_choice, moe_gain[None], added, total,
        quarter, experts, pieces,
    )
    arrived = lax.all_to_all(outgoing, EP, split_axis=0, concat_axis=0, tiled=True)
    hidden = norm_rows(moe_in, moe_gain)
    shared_gate = dot(hidden, w_sh_gate)
    shared_up = dot(hidden, w_sh_up)
    shared_act = (jax.nn.silu(shared_gate) * shared_up).astype(bf16)
    shared_part = dot(shared_act, w_sh_down).astype(bf16)
    arrived = after(arrived, shared_part)
    state_next = state_scan(arrived, pieces)
    top_far = shift_up(after(top_below, state_next))
    low_far = shift_down(after(low_above, state_next))
    state_start = lax.all_to_all(state_next, EP, split_axis=0, concat_axis=0, tiled=True)
    state_start = state_start.reshape(HEAD, -1)
    own, to_above, across_top, across_low, to_below = mixer_out(
        tp_rank.reshape(1), part, reach, state_start, head_gain[None], w_out, shared_part, tp_count
    )

    acts = hidden_units(
        arrived,
        [gate_own, gate_below, gate_above, gate_far],
        [up_own, up_below, up_above, up_far],
        pieces,
    )
    ready = results(
        acts,
        [down_own, top_below, low_below, top_above, low_above, top_far, low_far],
        experts,
    )
    returned = lax.all_to_all(ready, EP, split_axis=0, concat_axis=0, tiled=True)

    middle = across_top.shape[0]
    via_below = shift_up(across_top)
    via_above = shift_down(across_low)
    to_above = jnp.concatenate([to_above[:middle] + via_below, to_above[middle:]], axis=0)
    to_below = jnp.concatenate([to_below[:middle], to_below[middle:] + via_above], axis=0)
    from_below = shift_up(to_above)
    from_above = shift_down(to_below)
    total_rows = own.astype(f32) + from_below.astype(f32) + from_above.astype(f32)
    mixer_rows = mix_in.shape[0] // tp_count
    return (
        total_rows[:mixer_rows].astype(bf16),
        combine(returned, slot_ids, route_logit, total_rows[mixer_rows:]),
    )


def solution(mesh):
    finer = Mesh(mesh.devices.reshape(8, 4, 2, mesh.shape["tp"]), ("ep_0", "ep_1", "ep_2", "tp"))
    in_specs = (
        P(EP, None),
        P(EP),
        P(),
        P(None, "tp"),
        P(None, "tp"),
        P(None, "tp"),
        P("tp"),
        P("tp"),
        P("tp", None),
        P(EP, None),
        P(),
        P(EP, None),
        P(EP_TP, None),
        P(EP, None, "tp"),
        P(EP, None, "tp"),
        P(EP, "tp", None),
        P(None, "tp"),
        P(None, "tp"),
        P("tp", None),
    )
    out_specs = (P(EP_TP, None), P(EP_TP, None))

    return jax.shard_map(local, mesh=finer, in_specs=in_specs, out_specs=out_specs, check_vma=False)
```
